512 devices in a mesh: sp: 64 (over z, y), tp: 8 (over x, core).
Axes of the slice: x: 4, y: 4, z: 16, core: 2. Of those that a mesh axis runs over, the one named last changes fastest.
Arguments:
- tokens_in: bfloat16 [8192, 2048], P(('sp', 'tp')), may hold values from -9 to 9, as said below
- w_query: bfloat16 [2048, 2048], P(None, 'tp'), may hold values from -0.125 to 0.125
- w_key: bfloat16 [2048, 512], P(None, 'tp'), may hold values from -0.125 to 0.125
- w_value: bfloat16 [2048, 512], P(None, 'tp'), may hold values from -0.125 to 0.125
- w_out: bfloat16 [2048, 2048], P('tp'), may hold values from -0.125 to 0.125
- q_gain: float32 [64], replicated, may hold values from 0.1 to 14
- k_gain: float32 [64], replicated, may hold values from 0.1 to 14
Outputs:
- attended: bfloat16 [8192, 2048], P(('sp', 'tp'))
The draws below stay inside these ranges and needn't reach their ends.
Inputs may be any that keep to these rules, and one draw needn't show every extreme that they name: `tokens_in`: activations whose mean differs from one block of 128 tokens to another.
All inputs are finite; a program needn't handle non-finite values.
Results may differ from the reference program's by a relative error of at most 0.014.
The reference program's roundings to bfloat16 on the way (of `weights` and `mixed`) count: a program that leaves them out, or rounds other values in their place, can miss the bound.
Values may be sent and summed in bfloat16 or wider, within the bound.
No kernel may reach another device: no remote copies, remote signals or barrier semaphores. Data moves between devices by JAX's collectives and lax.ppermute only.
A program may use at most 64 MiB of HBM per device.

```python
import math
import jax
import jax.numpy as jnp
from jax import lax

D = 2048
HEADS = 32
KV_HEADS = 8
HD = 64
GRID_W = 64
TOK_DEV = 128
TOKENS = 8192
N_TP = 8


def draw_tokens_in(key, part):
    noise_key = jax.random.fold_in(key, 11)
    shift_key = jax.random.fold_in(key, 12)
    dir_key = jax.random.fold_in(key, 13)
    noise = jnp.clip(jax.random.normal(noise_key, (TOKENS, D), jnp.float32), -4.0, 4.0)
    shifts = jax.random.uniform(shift_key, (TOKENS // TOK_DEV, 1), jnp.float32, -1.5, 1.5)
    direction = jnp.clip(jax.random.normal(dir_key, (1, D), jnp.float32), -3.0, 3.0)
    offsets = jnp.repeat(shifts, TOK_DEV, axis=0) * direction
    return (noise + offsets).astype(jnp.bfloat16)


def gain_draw(key):
    return 1.0 + 0.18 * jnp.clip(jax.random.normal(key, (HD,), jnp.float32), -4.0, 4.0)


def draw_q_gain(key, part):
    return gain_draw(jax.random.fold_in(key, 21))


def draw_k_gain(key, part):
    return gain_draw(jax.random.fold_in(key, 22))


def block_levels(own_key, shape, pieces, least, top_value):
    def one(dim, blocks):
        steps = jax.random.uniform(jax.random.fold_in(jax.random.fold_in(own_key, 6), dim), (blocks,), jnp.float32, least / len(pieces), top_value / len(pieces))
        return jnp.repeat(jnp.exp(steps), shape[dim] // blocks).reshape((-1,) + (1,) * (len(shape) - dim - 1))

    level = one(*pieces[0])
    for cut in pieces[1:]:
        level = level * one(*cut)
    return level


def gaussian(rng, dims, scale, bound, cuts=(), kind=jnp.bfloat16):
    values = jax.random.normal(rng, dims, jnp.float32) * scale
    if len(cuts) > 0:
        values = block_levels(rng, dims, cuts, -0.22, 0.18) * values
    return jnp.clip(values, min=-bound, max=bound).astype(kind)


def setup_inputs(seed: int = 0) -> dict:
    key_of = jax.random.split(jax.random.key(seed), 8)
    tokens_in = draw_tokens_in(jax.random.fold_in(key_of[7], 71), 0)
    w_query = gaussian(key_of[1], (D, HEADS * HD), D ** -0.5, 0.125, ((1, 8),))
    w_key = gaussian(key_of[2], (D, KV_HEADS * HD), D ** -0.5, 0.125, ((1, 8),))
    w_value = gaussian(key_of[3], (D, KV_HEADS * HD), D ** -0.5, 0.125, ((1, 8),))
    w_out = gaussian(key_of[4], (HEADS * HD, D), (HEADS * HD) ** -0.5, 0.125, ((0, 8),))
    q_gain = draw_q_gain(jax.random.fold_in(key_of[7], 71), 0)
    k_gain = draw_k_gain(jax.random.fold_in(key_of[7], 71), 0)
    return {"tokens_in": tokens_in, "w_query": w_query, "w_key": w_key, "w_value": w_value, "w_out": w_out, "q_gain": q_gain, "k_gain": k_gain}


def turned(vectors, position, gain):
    pairs = vectors.shape[-1] // 4
    scaled = vectors * lax.rsqrt(lax.optimization_barrier(jnp.mean(vectors * vectors, axis=-1, keepdims=True)) + 1e-06) * gain
    freq = 10000.0 ** (-jnp.arange(pairs, dtype=jnp.float32) / pairs)
    grid_row = (position // GRID_W).astype(jnp.float32)
    grid_col = (position % GRID_W).astype(jnp.float32)
    angle = jnp.stack([grid_row[:, None] * freq, grid_col[:, None] * freq], axis=1)
    cosine = jnp.cos(angle)[:, None]
    sine = jnp.sin(angle)[:, None]
    split = scaled.reshape(scaled.shape[:-1] + (2, 2, pairs))
    first = split[..., 0, :]
    second = split[..., 1, :]
    joined = jnp.stack([first * cosine - second * sine, first * sine + second * cosine], axis=-2)
    return joined.reshape(scaled.shape)

def reference(tokens_in, w_query, w_key, w_value, w_out, q_gain, k_gain):
    head_dim = q_gain.shape[0]
    query = jnp.dot(tokens_in, w_query, preferred_element_type=jnp.float32).astype(jnp.bfloat16)
    key = jnp.dot(tokens_in, w_key, preferred_element_type=jnp.float32).astype(jnp.bfloat16)
    value = jnp.dot(tokens_in, w_value, preferred_element_type=jnp.float32).astype(jnp.bfloat16)
    position = jnp.arange(TOKENS, dtype=jnp.int32)
    group = HEADS // KV_HEADS
    query_n = turned(query.astype(jnp.float32).reshape(TOKENS, HEADS, head_dim), position, q_gain).astype(jnp.bfloat16)
    key_n = turned(key.astype(jnp.float32).reshape(TOKENS, KV_HEADS, head_dim), position, k_gain).astype(jnp.bfloat16)
    value_h = value.reshape(TOKENS, KV_HEADS, head_dim)
    block = math.gcd(TOKENS, 512)
    query_g = query_n.reshape(TOKENS // block, block, KV_HEADS, group, head_dim).transpose(2, 0, 3, 1, 4)
    keys_h = key_n.transpose(1, 0, 2)
    values_h = value_h.transpose(1, 0, 2)

    def one_head(packed):
        queries, keys, values = packed
        keys_f = keys.astype(jnp.float32)
        values_f = values.astype(jnp.float32)

        def one_block(qblock):
            scores = jnp.einsum('gqd,kd->gqk', qblock.astype(jnp.float32), keys_f) * head_dim ** (-0.5)
            peak = lax.optimization_barrier(jnp.max(scores, axis=-1, keepdims=True))
            expo = jnp.exp(scores - peak)
            total = lax.optimization_barrier(jnp.sum(expo, axis=-1, keepdims=True))
            weights = expo.astype(jnp.bfloat16).astype(jnp.float32)
            return (jnp.einsum('gqk,kd->gqd', weights, values_f) / total).astype(jnp.bfloat16)
        return lax.map(one_block, queries)
    mixed = lax.map(one_head, (query_g, keys_h, values_h))
    mixed = mixed.transpose(1, 3, 0, 2, 4).reshape(TOKENS, HEADS * head_dim)
    width = HEADS * head_dim // N_TP
    summed = jnp.zeros((TOKENS, w_out.shape[1]), jnp.float32)
    for index in range(N_TP):
        partial_value = jnp.dot(mixed[:, index * width:(index + 1) * width], w_out[index * width:(index + 1) * width], preferred_element_type=jnp.float32).astype(jnp.bfloat16)
        partial_value = lax.optimization_barrier(partial_value)
        summed = summed + partial_value.astype(jnp.float32)
    return summed.astype(jnp.bfloat16)
```

```python
import functools

import jax
import jax.numpy as jnp
from jax import lax
from jax.experimental import pallas as pl
from jax.experimental.pallas import tpu as pltpu
from jax.sharding import Mesh
from jax.sharding import PartitionSpec as P

F32, BF16 = jnp.float32, jnp.bfloat16
GRID_W = 64
SP = ("zq", "zp", "y")
TP = ("x", "c")
ALL = SP + TP
LOG2E = 1.4426950408889634
VMEM = pl.BlockSpec(memory_space=pltpu.VMEM)


def call(kernel, out, n_in, flops, byts, exps=0, limit=16, scratch=()):
    return pl.pallas_call(
        kernel,
        out_shape=out,
        in_specs=[VMEM] * n_in,
        out_specs=VMEM,
        scratch_shapes=list(scratch),
        compiler_params=pltpu.CompilerParams(vmem_limit_bytes=limit * 2**20),
        cost_estimate=pl.CostEstimate(flops=flops, bytes_accessed=byts, transcendentals=exps),
    )


def to_all(shard, axis):
    n = lax.axis_size(axis)
    return lax.all_to_all(
        jnp.broadcast_to(shard[None], (n, *shard.shape)), axis, 0, 0, tiled=True
    )


def turned(u, gain, tab):
    hd = u.shape[0]
    n = u * lax.rsqrt(jnp.sum(u * u, axis=0, keepdims=True) * (1.0 / hd) + 1e-6) * gain
    p = hd // 4
    out = []
    for half in range(2):
        a = n[half * 2 * p : half * 2 * p + p]
        b = n[half * 2 * p + p : half * 2 * p + 2 * p]
        cos, sin = tab[2 * half], tab[2 * half + 1]
        out += [a * cos - b * sin, a * sin + b * cos]
    return jnp.concatenate(out, axis=0)


def kv_kernel(copies, x_ref, wk_ref, wv_ref, gain_ref, tab_ref, out_ref):
    x = x_ref[...]
    k = jnp.dot(x, wk_ref[...], preferred_element_type=F32)
    v = jnp.dot(x, wv_ref[...], preferred_element_type=F32)
    kv = jnp.concatenate([k, v], axis=1).astype(BF16).astype(F32).T
    hd = k.shape[1]
    kt = turned(kv[:hd], gain_ref[...], tab_ref).astype(BF16)
    both = jnp.concatenate([kt, kv[hd:].astype(BF16)], axis=0)
    for i in range(copies):
        out_ref[i] = both


def q_kernel(copies, x_ref, w_ref, gain_ref, tab_ref, out_ref):
    q = jnp.dot(x_ref[...], w_ref[...], preferred_element_type=F32)
    qt = q.astype(BF16).astype(F32).T
    hd = gain_ref.shape[0]
    for h in range(qt.shape[0] // hd):
        rows = slice(h * hd, (h + 1) * hd)
        one = turned(qt[rows], gain_ref[...], tab_ref).astype(BF16)
        for i in range(copies):
            out_ref[i, rows] = one


def attend_kernel(hd, q_ref, kv_ref, out_ref, k_ref, v_ref):
    n_q, qc, rows = q_ref.shape
    n_k = kv_ref.shape[0]
    heads = qc // hd
    scale = hd**-0.5 * LOG2E
    for j in range(n_k):
        k_ref[j * rows : (j + 1) * rows, :] = kv_ref[j, :hd, :].astype(F32).T.astype(BF16)
        v_ref[16:, j * rows : (j + 1) * rows] = kv_ref[j, hd:, :]
    v_ref[:16, :] = jnp.ones((16, n_k * rows), BF16)

    def pair(i, _):
        tops, sums = [], []
        for h in range(heads):
            q = jnp.concatenate(
                [q_ref[2 * i + b, h * hd : (h + 1) * hd, :] for b in range(2)], axis=1
            )
            s = jnp.dot(k_ref[...], q, preferred_element_type=F32)
            top = (jnp.max(s, axis=0, keepdims=True) * scale).astype(BF16).astype(F32)
            p = jnp.exp2(s * scale - top).astype(BF16)
            o = jnp.dot(v_ref[...], p, preferred_element_type=F32)
            tops.append(top)
            sums.append(o[:1])
            for b in range(2):
                out_ref[2 * i + b, h * hd : (h + 1) * hd, :] = o[
                    16:, b * rows : (b + 1) * rows
                ].astype(BF16)
        total = jnp.concatenate(sums, axis=0)
        hi = total.astype(BF16).astype(F32)
        stats = jnp.concatenate(tops + [hi, total - hi, jnp.zeros_like(total)], axis=0).astype(BF16)
        for b in range(2):
            out_ref[2 * i + b, qc:, :] = stats[:, b * rows : (b + 1) * rows]
        return 0

    lax.fori_loop(0, n_q // 2, pair, 0)


def mix_kernel(hd, n_tp, got_ref, w_ref, out_ref, mixed_ref):
    parts, _, rows = got_ref.shape
    qc = w_ref.shape[0]
    heads = qc // hd
    st = [got_ref[i, qc:, :].astype(F32) for i in range(parts)]
    top = functools.reduce(jnp.maximum, [s[:heads] for s in st])
    factor = [jnp.exp2(s[:heads] - top) for s in st]
    total = functools.reduce(
        jnp.add,
        [f * (s[heads : 2 * heads] + s[2 * heads : 3 * heads]) for f, s in zip(factor, st)],
    )
    for h in range(heads):
        acc = 0.0
        for i in range(parts):
            acc += got_ref[i, h * hd : (h + 1) * hd, :].astype(F32) * factor[i][h : h + 1]
        mixed_ref[h * hd : (h + 1) * hd, :] = acc / total[h : h + 1]
    mixed = mixed_ref[...].T.astype(BF16)
    out = jnp.dot(mixed, w_ref[...], preferred_element_type=F32).astype(BF16)
    each = rows // n_tp
    for t in range(n_tp):
        out_ref[t % 2, t // 2] = out[t * each : (t + 1) * each]


def body(tokens_in, w_query, w_key, w_value, w_out, q_gain, k_gain):
    hd = q_gain.shape[0]
    qc = w_query.shape[1]
    mine, d = tokens_in.shape
    n_tp = lax.axis_size(TP)
    rows = mine * n_tp
    n_k = lax.axis_size("zq")
    n_q = lax.axis_size(("zp", "y"))
    heads = qc // hd

    tokens = to_all(tokens_in, TP).reshape(rows, d)
    position = lax.axis_index(SP) * rows + jnp.arange(rows, dtype=jnp.int32)
    pairs = hd // 4
    freq = 10000.0 ** (-jnp.arange(pairs, dtype=F32) / pairs)
    grid = jnp.stack([position // GRID_W, position % GRID_W]).astype(F32)
    angle = grid[:, None, :] * freq[None, :, None]
    tab = jnp.stack([jnp.cos(angle), jnp.sin(angle)], axis=1).reshape(4, pairs, rows)
    gains = [jnp.broadcast_to(g[:, None], (hd, rows)) for g in (q_gain, k_gain)]

    kv = call(
        functools.partial(kv_kernel, n_k),
        jax.ShapeDtypeStruct((n_k, 2 * hd, rows), BF16),
        5,
        2 * rows * d * 2 * hd,
        2 * d * (rows + 2 * hd),
    )(tokens, w_key, w_value, gains[1], tab)
    kv = lax.all_to_all(kv, "zq", 0, 0, tiled=True)

    query = call(
        functools.partial(q_kernel, n_q),
        jax.ShapeDtypeStruct((n_q, qc, rows), BF16),
        4,
        2 * rows * d * qc,
        2 * d * (rows + qc),
    )(tokens, w_query, gains[0], tab)
    query = lax.all_to_all(query, ("zp", "y"), 0, 0, tiled=True)

    part = call(
        functools.partial(attend_kernel, hd),
        jax.ShapeDtypeStruct((n_q, qc + 16, rows), BF16),
        2,
        4 * heads * n_q * rows * n_k * rows * hd,
        4 * n_q * qc * rows,
        exps=heads * n_q * rows * n_k * rows,
        limit=32,
        scratch=(
            pltpu.VMEM((n_k * rows, hd), BF16),
            pltpu.VMEM((hd + 16, n_k * rows), BF16),
        ),
    )(query, kv)
    got = lax.all_to_all(part, ("zp", "y"), 0, 0, tiled=True)

    partial = call(
        functools.partial(mix_kernel, hd, n_tp),
        jax.ShapeDtypeStruct((2, n_tp // 2, mine, d), BF16),
        2,
        2 * rows * qc * d,
        2 * d * (rows + qc),
        scratch=(pltpu.VMEM((qc, rows), F32),),
    )(got, w_out)
    near = lax.all_to_all(partial, "c", 0, 0, tiled=True)
    near = near.astype(F32).sum(axis=0).astype(BF16)
    far = lax.all_to_all(near, "x", 0, 0, tiled=True)
    return far.astype(F32).sum(axis=0).astype(BF16)


def solution(mesh):
    finer = Mesh(mesh.devices.reshape(8, 2, 4, mesh.shape["tp"] // 2, 2), ALL)
    return jax.shard_map(
        body,
        mesh=finer,
        in_specs=(
            P(ALL, None),
            P(None, TP),
            P(None, TP),
            P(None, TP),
            P(TP, None),
            P(),
            P(),
        ),
        out_specs=P(ALL, None),
        check_vma=False,
    )
```

```python
import functools

import jax
import jax.numpy as jnp
from jax import lax
from jax.experimental import pallas as pl
from jax.experimental.pallas import tpu as pltpu
from jax.sharding import Mesh
from jax.sharding import PartitionSpec as P


F32, BF16 = jnp.float32, jnp.bfloat16
GRID_W = 64
SP = ("zq", "zp", "y")
TP = ("x", "c")
ALL = SP + TP
LOG2E = 1.4426950408889634
VMEM = pl.BlockSpec(memory_space=pltpu.VMEM)


def call(kernel, out, n_in, flops, byts, exps=0, limit=16, scratch=()):
    return pl.pallas_call(
        kernel,
        out_shape=out,
        in_specs=[VMEM] * n_in,
        out_specs=VMEM,
        scratch_shapes=list(scratch),
        compiler_params=pltpu.CompilerParams(vmem_limit_bytes=limit * 2**20),
        cost_estimate=pl.CostEstimate(flops=flops, bytes_accessed=byts, transcendentals=exps),
    )


def to_all(shard, axis):
    n = lax.axis_size(axis)
    return lax.all_to_all(
        jnp.broadcast_to(shard[None], (n, *shard.shape)), axis, 0, 0, tiled=True
    )


def table_kernel(qg_ref, kg_ref, tab_ref, out_ref):
    p = tab_ref.shape[1]
    for i, ref in enumerate((qg_ref, kg_ref)):
        gain = jnp.broadcast_to(ref[...], (tab_ref.shape[2], ref.shape[1])).T
        for half in range(2):
            cos, sin = tab_ref[2 * half], tab_ref[2 * half + 1]
            a, b = 2 * half * p, (2 * half + 1) * p
            ga, gb = gain[a : a + p], gain[b : b + p]
            out_ref[i, 0, a : a + p] = ga * cos
            out_ref[i, 0, b : b + p] = gb * cos
            out_ref[i, 1, a : a + p] = -gb * sin
            out_ref[i, 1, b : b + p] = ga * sin


def turned(u, cos, sin):
    hd = u.shape[0]
    p = hd // 4
    swapped = jnp.concatenate([u[p : 2 * p], u[:p], u[3 * p :], u[2 * p : 3 * p]], axis=0)
    inv = lax.rsqrt(jnp.sum(u * u, axis=0, keepdims=True) * (1.0 / hd) + 1e-6)
    return (u * inv) * cos + (swapped * inv) * sin


NT = (((1,), (1,)), ((), ()))


def kv_kernel(copies, x_ref, wk_ref, wv_ref, tab_ref, out_ref):
    x = x_ref[...]
    k = lax.dot_general(wk_ref[...], x, NT, preferred_element_type=F32)
    v = lax.dot_general(wv_ref[...], x, NT, preferred_element_type=F32)
    kt = turned(k.astype(BF16).astype(F32), tab_ref[1, 0], tab_ref[1, 1]).astype(BF16)
    both = jnp.concatenate([kt, v.astype(BF16)], axis=0)
    for i in range(copies):
        out_ref[i] = both


def q_kernel(x_ref, w_ref, tab_ref, out_ref):
    q = jnp.dot(x_ref[...], w_ref[...], preferred_element_type=F32)
    qt = q.astype(BF16).astype(F32).T
    hd = tab_ref.shape[2]
    for h in range(qt.shape[0] // hd):
        rows = slice(h * hd, (h + 1) * hd)
        out_ref[0, rows] = turned(qt[rows], tab_ref[0, 0], tab_ref[0, 1]).astype(BF16)


def pair_kernel(hd, q_ref, out_ref):
    n_q, qc, rows = q_ref.shape
    for i in range(n_q):
        for h in range(qc // hd):
            out_ref[i // 2, h, :, (i % 2) * rows : (i % 2 + 1) * rows] = q_ref[
                i, h * hd : (h + 1) * hd, :
            ]


def attend_kernel(hd, q_ref, kv_ref, out_ref, k_ref, v_ref):
    n_pair, heads, _, rows = q_ref.shape
    rows //= 2
    n_k = kv_ref.shape[0]
    qc = heads * hd
    scale = hd**-0.5 * LOG2E
    for j in range(n_k):
        k_ref[j * rows : (j + 1) * rows, :] = kv_ref[j, :hd, :].astype(F32).T.astype(BF16)
        v_ref[16:, j * rows : (j + 1) * rows] = kv_ref[j, hd:, :]
    v_ref[:16, :] = jnp.ones((16, n_k * rows), BF16)

    def pair(i, _):
        tops, sums = [], []
        for h in range(heads):
            s = jnp.dot(k_ref[...], q_ref[i, h], preferred_element_type=F32)
            top = (jnp.max(s, axis=0, keepdims=True) * scale).astype(BF16).astype(F32)
            p = jnp.exp2(s * scale - top).astype(BF16)
            o = jnp.dot(v_ref[...], p, preferred_element_type=F32)
            tops.append(top)
            sums.append(o[:1])
            for b in range(2):
                out_ref[2 * i + b, h * hd : (h + 1) * hd, :] = o[
                    16:, b * rows : (b + 1) * rows
                ].astype(BF16)
        total = jnp.concatenate(sums, axis=0)
        hi = total.astype(BF16).astype(F32)
        stats = jnp.concatenate(tops + [hi, total - hi, jnp.zeros_like(total)], axis=0).astype(BF16)
        for b in range(2):
            out_ref[2 * i + b, qc:, :] = stats[:, b * rows : (b + 1) * rows]
        return 0

    lax.fori_loop(0, n_pair, pair, 0)


def mix_kernel(hd, n_tp, got_ref, w_ref, out_ref, mixed_ref):
    parts, _, rows = got_ref.shape
    qc = w_ref.shape[0]
    heads = qc // hd
    st = [got_ref[i, qc:, :].astype(F32) for i in range(parts)]
    top = functools.reduce(jnp.maximum, [s[:heads] for s in st])
    factor = [jnp.exp2(s[:heads] - top) for s in st]
    total = functools.reduce(
        jnp.add,
        [f * (s[heads : 2 * heads] + s[2 * heads : 3 * heads]) for f, s in zip(factor, st)],
    )
    for h in range(heads):
        acc = 0.0
        for i in range(parts):
            acc += got_ref[i, h * hd : (h + 1) * hd, :].astype(F32) * factor[i][h : h + 1]
        mixed_ref[h * hd : (h + 1) * hd, :] = acc / total[h : h + 1]
    mixed = mixed_ref[...].T.astype(BF16)
    out = jnp.dot(mixed, w_ref[...], preferred_element_type=F32).astype(BF16)
    each = rows // n_tp
    for t in range(n_tp):
        out_ref[t] = out[t * each : (t + 1) * each]


def body(tokens_in, w_query, w_key, w_value, w_out, q_gain, k_gain):
    hd = q_gain.shape[0]
    qc = w_query.shape[1]
    mine, d = tokens_in.shape
    n_tp = lax.axis_size(TP)
    rows = mine * n_tp
    n_k = lax.axis_size("zq")
    n_q = lax.axis_size(("zp", "y"))
    heads = qc // hd

    position = lax.axis_index(SP) * rows + jnp.arange(rows, dtype=jnp.int32)
    pairs = hd // 4
    freq = 10000.0 ** (-jnp.arange(pairs, dtype=F32) / pairs)
    grid = jnp.stack([position // GRID_W, position % GRID_W]).astype(F32)
    angle = grid[:, None, :] * freq[None, :, None]
    tab = jnp.stack([jnp.cos(angle), jnp.sin(angle)], axis=1).reshape(4, pairs, rows)
    tab = call(
        table_kernel,
        jax.ShapeDtypeStruct((2, 2, hd, rows), F32),
        3,
        8 * hd * rows,
        32 * hd * rows,
    )(q_gain[None], k_gain[None], tab)
    tokens_in, tab = lax.optimization_barrier((tokens_in, tab))
    tokens = to_all(tokens_in, TP).reshape(rows, d)

    kv = call(
        functools.partial(kv_kernel, n_k),
        jax.ShapeDtypeStruct((n_k, 2 * hd, rows), BF16),
        4,
        2 * rows * d * 2 * hd,
        2 * d * (rows + 2 * hd),
    )(tokens, w_key.T, w_value.T, tab)
    kv = lax.all_to_all(kv, "zq", 0, 0, tiled=True)

    query = call(
        q_kernel,
        jax.ShapeDtypeStruct((1, qc, rows), BF16),
        3,
        2 * rows * d * qc,
        2 * d * (rows + qc),
    )(tokens, w_query, tab)
    query = lax.all_gather(query, ("zp", "y"), axis=0, tiled=True)
    query = call(
        functools.partial(pair_kernel, hd),
        jax.ShapeDtypeStruct((n_q // 2, heads, hd, 2 * rows), BF16),
        1,
        n_q * qc * rows,
        4 * n_q * qc * rows,
    )(query)

    part = call(
        functools.partial(attend_kernel, hd),
        jax.ShapeDtypeStruct((n_q, qc + 16, rows), BF16),
        2,
        4 * heads * n_q * rows * n_k * rows * hd,
        4 * n_q * qc * rows,
        exps=heads * n_q * rows * n_k * rows,
        limit=32,
        scratch=(
            pltpu.VMEM((n_k * rows, hd), BF16),
            pltpu.VMEM((hd + 16, n_k * rows), BF16),
        ),
    )(query, kv)
    got = lax.all_to_all(part, ("zp", "y"), 0, 0, tiled=True)

    partial = call(
        functools.partial(mix_kernel, hd, n_tp),
        jax.ShapeDtypeStruct((n_tp, mine, d), BF16),
        2,
        2 * rows * qc * d,
        2 * d * (rows + qc),
        scratch=(pltpu.VMEM((qc, rows), F32),),
    )(got, w_out)
    got = lax.all_to_all(partial, TP, 0, 0, tiled=True)
    return got.astype(F32).sum(axis=0).astype(BF16)


def solution(mesh):
    finer = Mesh(mesh.devices.reshape(8, 2, 4, mesh.shape["tp"] // 2, 2), ALL)

    return jax.shard_map(
        body,
        mesh=finer,
        in_specs=(
            P(ALL, None),
            P(None, TP),
            P(None, TP),
            P(None, TP),
            P(TP, None),
            P(),
            P(),
        ),
        out_specs=P(ALL, None),
        check_vma=False,
    )
```

```python
import functools

import jax
import jax.numpy as jnp
from jax import lax
from jax.experimental import pallas as pl
from jax.experimental.pallas import tpu as pltpu
from jax.sharding import Mesh
from jax.sharding import PartitionSpec as P


F32, BF16 = jnp.float32, jnp.bfloat16
GRID_W = 64
SP = ("zq", "zp", "y")
TP = ("x", "c")
ALL = SP + TP
LOG2E = 1.4426950408889634
VMEM = pl.BlockSpec(memory_space=pltpu.VMEM)


def call(kernel, out, n_in, flops, byts, exps=0, limit=16, scratch=()):
    return pl.pallas_call(
        kernel,
        out_shape=out,
        in_specs=[VMEM] * n_in,
        out_specs=VMEM,
        scratch_shapes=list(scratch),
        compiler_params=pltpu.CompilerParams(vmem_limit_bytes=limit * 2**20),
        cost_estimate=pl.CostEstimate(flops=flops, bytes_accessed=byts, transcendentals=exps),
    )


def to_all(shard, axis):
    n = lax.axis_size(axis)
    return lax.all_to_all(
        jnp.broadcast_to(shard[None], (n, *shard.shape)), axis, 0, 0, tiled=True
    )


def table_kernel(qg_ref, kg_ref, tab_ref, out_ref):
    p = tab_ref.shape[1]
    for i, ref in enumerate((qg_ref, kg_ref)):
        gain = jnp.broadcast_to(ref[...], (tab_ref.shape[2], ref.shape[1])).T
        for half in range(2):
            cos, sin = tab_ref[2 * half], tab_ref[2 * half + 1]
            a, b = 2 * half * p, (2 * half + 1) * p
            ga, gb = gain[a : a + p], gain[b : b + p]
            out_ref[i, 0, a : a + p] = ga * cos
            out_ref[i, 0, b : b + p] = gb * cos
            out_ref[i, 1, a : a + p] = -gb * sin
            out_ref[i, 1, b : b + p] = ga * sin


def turned(u, cos, sin):
    hd = u.shape[0]
    p = hd // 4
    swapped = jnp.concatenate([u[p : 2 * p], u[:p], u[3 * p :], u[2 * p : 3 * p]], axis=0)
    inv = lax.rsqrt(jnp.sum(u * u, axis=0, keepdims=True) * (1.0 / hd) + 1e-6)
    return (u * inv) * cos + (swapped * inv) * sin


NT = (((1,), (1,)), ((), ()))


def kv_kernel(copies, x_ref, wk_ref, wv_ref, tab_ref, out_ref):
    x = x_ref[...]
    k = lax.dot_general(wk_ref[...], x, NT, preferred_element_type=F32)
    v = lax.dot_general(wv_ref[...], x, NT, preferred_element_type=F32)
    kt = turned(k.astype(BF16).astype(F32), tab_ref[1, 0], tab_ref[1, 1]).astype(BF16)
    both = jnp.concatenate([kt, v.astype(BF16)], axis=0)
    for i in range(copies):
        out_ref[i] = both


def q_kernel(x_ref, w_ref, tab_ref, out_ref):
    q = jnp.dot(x_ref[...], w_ref[...], preferred_element_type=F32)
    qt = q.astype(BF16).astype(F32).T
    hd = tab_ref.shape[2]
    for h in range(qt.shape[0] // hd):
        rows = slice(h * hd, (h + 1) * hd)
        out_ref[rows] = turned(qt[rows], tab_ref[0, 0], tab_ref[0, 1]).astype(BF16)


def pair_kernel(hd, zp_ref, q_ref, out_ref):
    n_q, qc, rows = q_ref.shape
    for i in range(n_q // 2):
        for b in range(2):
            block = 2 * i + (zp_ref[0] + b) % 2
            for h in range(qc // hd):
                out_ref[i, h, :, b * rows : (b + 1) * rows] = q_ref[
                    block, h * hd : (h + 1) * hd, :
                ]


def attend_kernel(hd, q_ref, kv_ref, out_ref, k_ref, v_ref):
    n_pair, heads, _, rows = q_ref.shape
    rows //= 2
    n_k = kv_ref.shape[0]
    qc = heads * hd
    scale = hd**-0.5 * LOG2E
    for j in range(n_k):
        k_ref[j * rows : (j + 1) * rows, :] = kv_ref[j, :hd, :].astype(F32).T.astype(BF16)
        v_ref[16:, j * rows : (j + 1) * rows] = kv_ref[j, hd:, :]
    v_ref[:16, :] = jnp.ones((16, n_k * rows), BF16)

    def pair(i, _):
        tops, sums = [], []
        for h in range(heads):
            s = jnp.dot(k_ref[...], q_ref[i, h], preferred_element_type=F32)
            top = (jnp.max(s, axis=0, keepdims=True) * scale).astype(BF16).astype(F32)
            p = jnp.exp2(s * scale - top).astype(BF16)
            o = jnp.dot(v_ref[...], p, preferred_element_type=F32)
            tops.append(top)
            sums.append(o[:1])
            for b in range(2):
                out_ref[2 * i + b, h * hd : (h + 1) * hd, :] = o[
                    16:, b * rows : (b + 1) * rows
                ].astype(BF16)
        total = jnp.concatenate(sums, axis=0)
        hi = total.astype(BF16).astype(F32)
        stats = jnp.concatenate(tops + [hi, total - hi, jnp.zeros_like(total)], axis=0).astype(BF16)
        for b in range(2):
            out_ref[2 * i + b, qc:, :] = stats[:, b * rows : (b + 1) * rows]
        return 0

    lax.fori_loop(0, n_pair, pair, 0)


def mix_kernel(hd, n_tp, got_ref, w_ref, out_ref, mixed_ref):
    parts, _, rows = got_ref.shape
    qc = w_ref.shape[0]
    heads = qc // hd
    st = [got_ref[i, qc:, :].astype(F32) for i in range(parts)]
    top = functools.reduce(jnp.maximum, [s[:heads] for s in st])
    factor = [jnp.exp2(s[:heads] - top) for s in st]
    total = functools.reduce(
        jnp.add,
        [f * (s[heads : 2 * heads] + s[2 * heads : 3 * heads]) for f, s in zip(factor, st)],
    )
    for h in range(heads):
        acc = 0.0
        for i in range(parts):
            acc += got_ref[i, h * hd : (h + 1) * hd, :].astype(F32) * factor[i][h : h + 1]
        mixed_ref[h * hd : (h + 1) * hd, :] = acc / total[h : h + 1]
    mixed = mixed_ref[...].T.astype(BF16)
    out = jnp.dot(mixed, w_ref[...], preferred_element_type=F32).astype(BF16)
    each = rows // n_tp
    for t in range(n_tp):
        out_ref[t] = out[t * each : (t + 1) * each]


def body(tokens_in, w_query, w_key, w_value, w_out, q_gain, k_gain):
    hd = q_gain.shape[0]
    qc = w_query.shape[1]
    mine, d = tokens_in.shape
    n_tp = lax.axis_size(TP)
    rows = mine * n_tp
    n_k = lax.axis_size("zq")
    n_q = lax.axis_size(("zp", "y"))
    heads = qc // hd

    position = lax.axis_index(SP) * rows + jnp.arange(rows, dtype=jnp.int32)
    pairs = hd // 4
    freq = 10000.0 ** (-jnp.arange(pairs, dtype=F32) / pairs)
    grid = jnp.stack([position // GRID_W, position % GRID_W]).astype(F32)
    angle = grid[:, None, :] * freq[None, :, None]
    tab = jnp.stack([jnp.cos(angle), jnp.sin(angle)], axis=1).reshape(4, pairs, rows)
    tab = call(
        table_kernel,
        jax.ShapeDtypeStruct((2, 2, hd, rows), F32),
        3,
        8 * hd * rows,
        32 * hd * rows,
    )(q_gain[None], k_gain[None], tab)
    tokens_in, tab = lax.optimization_barrier((tokens_in, tab))
    tokens = to_all(tokens_in, TP).reshape(rows, d)

    query = call(
        q_kernel,
        jax.ShapeDtypeStruct((qc, rows), BF16),
        3,
        2 * rows * d * qc,
        2 * d * (rows + qc),
    )(tokens, w_query, tab)
    other = lax.ppermute(query, "zp", [(0, 1), (1, 0)])
    kv = call(
        functools.partial(kv_kernel, n_k),
        jax.ShapeDtypeStruct((n_k, 2 * hd, rows), BF16),
        4,
        2 * rows * d * 2 * hd,
        2 * d * (rows + 2 * hd),
    )(tokens, w_key.T, w_value.T, tab)
    kv = lax.all_to_all(kv, "zq", 0, 0, tiled=True)
    query = lax.all_gather(jnp.stack([query, other]), "y", axis=0, tiled=True)
    query = pl.pallas_call(
        functools.partial(pair_kernel, hd),
        out_shape=jax.ShapeDtypeStruct((n_q // 2, heads, hd, 2 * rows), BF16),
        in_specs=[pl.BlockSpec(memory_space=pltpu.SMEM), VMEM],
        out_specs=VMEM,
        compiler_params=pltpu.CompilerParams(vmem_limit_bytes=16 * 2**20),
        cost_estimate=pl.CostEstimate(
            flops=n_q * qc * rows, bytes_accessed=4 * n_q * qc * rows, transcendentals=0
        ),
    )(lax.axis_index("zp").astype(jnp.int32)[None], query)

    part = call(
        functools.partial(attend_kernel, hd),
        jax.ShapeDtypeStruct((n_q, qc + 16, rows), BF16),
        2,
        4 * heads * n_q * rows * n_k * rows * hd,
        4 * n_q * qc * rows,
        exps=heads * n_q * rows * n_k * rows,
        limit=32,
        scratch=(
            pltpu.VMEM((n_k * rows, hd), BF16),
            pltpu.VMEM((hd + 16, n_k * rows), BF16),
        ),
    )(query, kv)
    got = lax.all_to_all(part, ("y", "zp"), 0, 0, tiled=True)

    partial = call(
        functools.partial(mix_kernel, hd, n_tp),
        jax.ShapeDtypeStruct((n_tp, mine, d), BF16),
        2,
        2 * rows * qc * d,
        2 * d * (rows + qc),
        scratch=(pltpu.VMEM((qc, rows), F32),),
    )(got, w_out)
    got = lax.all_to_all(partial, TP, 0, 0, tiled=True)
    return got.astype(F32).sum(axis=0).astype(BF16)


def solution(mesh):
    finer = Mesh(mesh.devices.reshape(8, 2, 4, mesh.shape["tp"] // 2, 2), ALL)

    return jax.shard_map(
        body,
        mesh=finer,
        in_specs=(
            P(ALL, None),
            P(None, TP),
            P(None, TP),
            P(None, TP),
            P(TP, None),
            P(),
            P(),
        ),
        out_specs=P(ALL, None),
        check_vma=False,
    )
```

```python
import functools

import jax
import jax.numpy as jnp
from jax import lax
from jax.experimental import pallas as pl
from jax.experimental.pallas import tpu as pltpu
from jax.sharding import Mesh
from jax.sharding import PartitionSpec as P


F32, BF16 = jnp.float32, jnp.bfloat16
GRID_W = 64
SP = ("zq", "zp", "y")
TP = ("x", "c")
ALL = SP + TP
LOG2E = 1.4426950408889634
VMEM = pl.BlockSpec(memory_space=pltpu.VMEM)


def call(kernel, out, n_in, flops, byts, exps=0, limit=16, scratch=()):
    return pl.pallas_call(
        kernel,
        out_shape=out,
        in_specs=[VMEM] * n_in,
        out_specs=VMEM,
        scratch_shapes=list(scratch),
        compiler_params=pltpu.CompilerParams(vmem_limit_bytes=limit * 2**20),
        cost_estimate=pl.CostEstimate(flops=flops, bytes_accessed=byts, transcendentals=exps),
    )


def tables(gain, tab_ref):
    p = tab_ref.shape[1]
    gain = jnp.broadcast_to(gain, (tab_ref.shape[2], gain.shape[1])).T
    cosines, sines = [], []
    for half in range(2):
        cos, sin = tab_ref[2 * half], tab_ref[2 * half + 1]
        ga = gain[2 * half * p : (2 * half + 1) * p]
        gb = gain[(2 * half + 1) * p : (2 * half + 2) * p]
        cosines += [ga * cos, gb * cos]
        sines += [-gb * sin, ga * sin]
    return jnp.concatenate(cosines, axis=0), jnp.concatenate(sines, axis=0)


def turned(u, cos, sin):
    hd = u.shape[0]
    p = hd // 4
    swapped = jnp.concatenate([u[p : 2 * p], u[:p], u[3 * p :], u[2 * p : 3 * p]], axis=0)
    inv = lax.rsqrt(jnp.sum(u * u, axis=0, keepdims=True) * (1.0 / hd) + 1e-6)
    return (u * inv) * cos + (swapped * inv) * sin


NT = (((1,), (1,)), ((), ()))


def in_order(x_ref):
    n = x_ref.shape[0]
    return jnp.concatenate([x_ref[(t % 2) * (n // 2) + t // 2] for t in range(n)], axis=0)


def kv_kernel(copies, x_ref, wk_ref, wv_ref, gain_ref, tab_ref, out_ref):
    x = in_order(x_ref)
    k = lax.dot_general(wk_ref[...], x, NT, preferred_element_type=F32)
    v = lax.dot_general(wv_ref[...], x, NT, preferred_element_type=F32)
    kt = turned(k.astype(BF16).astype(F32), *tables(gain_ref[1:2], tab_ref)).astype(BF16)
    both = jnp.concatenate([kt, v.astype(BF16)], axis=0)
    for i in range(copies):
        out_ref[i] = both


def q_kernel(x_ref, w_ref, gain_ref, tab_ref, out_ref):
    q = jnp.dot(in_order(x_ref), w_ref[...], preferred_element_type=F32)
    qt = q.astype(BF16).astype(F32).T
    hd = gain_ref.shape[1]
    both = tables(gain_ref[0:1], tab_ref)
    for h in range(qt.shape[0] // hd):
        rows = slice(h * hd, (h + 1) * hd)
        out_ref[rows] = turned(qt[rows], *both).astype(BF16)


def pair_kernel(hd, zp_ref, q_ref, out_ref):
    n_q, qc, rows = q_ref.shape
    for i in range(n_q // 2):
        for b in range(2):
            block = 2 * i + (zp_ref[0] + b) % 2
            for h in range(qc // hd):
                out_ref[i, h, :, b * rows : (b + 1) * rows] = q_ref[
                    block, h * hd : (h + 1) * hd, :
                ]


def attend_kernel(hd, q_ref, kv_ref, out_ref, k_ref, v_ref, s_ref):
    n_pair, heads, _, rows = q_ref.shape
    rows //= 2
    n_k = kv_ref.shape[0]
    n_keys = n_k * rows
    qc = heads * hd
    step = n_keys // 2
    scale = hd**-0.5 * LOG2E
    for j in range(n_k):
        k_ref[j * rows : (j + 1) * rows, :] = kv_ref[j, :hd, :].astype(F32).T.astype(BF16)
        v_ref[16:, j * rows : (j + 1) * rows] = kv_ref[j, hd:, :]
    v_ref[:16, :] = jnp.ones((16, n_keys), BF16)

    def score(i, h, slot):
        top = None
        for c in range(0, n_keys, step):
            s = jnp.dot(k_ref[c : c + step, :], q_ref[i, h], preferred_element_type=F32)
            s_ref[slot, c : c + step] = s
            part = jnp.max(s.reshape(step // 8, 8, 2 * rows), axis=0)
            top = part if top is None else jnp.maximum(top, part)
        return (jnp.max(top, axis=0, keepdims=True) * scale).astype(BF16).astype(F32)

    def pair(i, top):
        tops, sums = [], []
        for h in range(heads):
            if h + 1 < heads:
                later = score(i, h + 1, (h + 1) % 2)
            else:
                later = score(jnp.minimum(i + 1, n_pair - 1), 0, 0)
            o = 0.0
            for c in range(0, n_keys, step):
                p = jnp.exp2(s_ref[h % 2, c : c + step] * scale - top).astype(BF16)
                o += jnp.dot(v_ref[:, c : c + step], p, preferred_element_type=F32)
            tops.append(top)
            sums.append(o[:1])
            for b in range(2):
                out_ref[2 * i + b, h * hd : (h + 1) * hd, :] = o[
                    16:, b * rows : (b + 1) * rows
                ].astype(BF16)
            top = later
        total = jnp.concatenate(sums, axis=0)
        hi = total.astype(BF16).astype(F32)
        stats = jnp.concatenate(tops + [hi, total - hi, jnp.zeros_like(total)], axis=0).astype(BF16)
        for b in range(2):
            out_ref[2 * i + b, qc:, :] = stats[:, b * rows : (b + 1) * rows]
        return top

    lax.fori_loop(0, n_pair, pair, score(0, 0, 0))


def mix_kernel(hd, n_tp, got_ref, w_ref, out_ref, mixed_ref):
    parts, _, rows = got_ref.shape
    qc = w_ref.shape[0]
    heads = qc // hd
    st = [got_ref[i, qc:, :].astype(F32) for i in range(parts)]
    top = functools.reduce(jnp.maximum, [s[:heads] for s in st])
    factor = [jnp.exp2(s[:heads] - top) for s in st]
    total = functools.reduce(
        jnp.add,
        [f * (s[heads : 2 * heads] + s[2 * heads : 3 * heads]) for f, s in zip(factor, st)],
    )
    for h in range(heads):
        acc = 0.0
        for i in range(parts):
            acc += got_ref[i, h * hd : (h + 1) * hd, :].astype(F32) * factor[i][h : h + 1]
        mixed_ref[h * hd : (h + 1) * hd, :] = acc / total[h : h + 1]
    mixed = mixed_ref[...].T.astype(BF16)
    out = jnp.dot(mixed, w_ref[...], preferred_element_type=F32).astype(BF16)
    each = rows // n_tp
    for t in range(n_tp):
        out_ref[t] = out[t * each : (t + 1) * each]


def body(tokens_in, w_query, w_key, w_value, w_out, q_gain, k_gain):
    hd = q_gain.shape[0]
    qc = w_query.shape[1]
    mine, d = tokens_in.shape
    n_tp = lax.axis_size(TP)
    rows = mine * n_tp
    n_k = lax.axis_size("zq")
    n_q = lax.axis_size(("zp", "y"))
    heads = qc // hd

    position = lax.axis_index(SP) * rows + jnp.arange(rows, dtype=jnp.int32)
    pairs = hd // 4
    freq = 10000.0 ** (-jnp.arange(pairs, dtype=F32) / pairs)
    grid = jnp.stack([position // GRID_W, position % GRID_W]).astype(F32)
    angle = grid[:, None, :] * freq[None, :, None]
    tab = jnp.stack([jnp.cos(angle), jnp.sin(angle)], axis=1).reshape(4, pairs, rows)
    gains = jnp.stack([q_gain, k_gain])
    tokens_in, tab, gains = lax.optimization_barrier((tokens_in, tab, gains))
    sent = jnp.broadcast_to(tokens_in[None], (lax.axis_size("x"), mine, d))
    tokens = lax.all_to_all(sent, "x", 0, 0, tiled=True)
    tokens = lax.all_gather(tokens, "c", axis=0).reshape(n_tp, mine, d)

    query = call(
        q_kernel,
        jax.ShapeDtypeStruct((qc, rows), BF16),
        4,
        2 * rows * d * qc,
        2 * d * (rows + qc),
    )(tokens, w_query, gains, tab)
    other = lax.ppermute(query, "zp", [(0, 1), (1, 0)])
    kv = call(
        functools.partial(kv_kernel, n_k),
        jax.ShapeDtypeStruct((n_k, 2 * hd, rows), BF16),
        5,
        2 * rows * d * 2 * hd,
        2 * d * (rows + 2 * hd),
    )(tokens, w_key.T, w_value.T, gains, tab)
    kv = lax.all_to_all(kv, "zq", 0, 0, tiled=True)
    query = lax.all_gather(jnp.stack([query, other]), "y", axis=0, tiled=True)
    query = pl.pallas_call(
        functools.partial(pair_kernel, hd),
        out_shape=jax.ShapeDtypeStruct((n_q // 2, heads, hd, 2 * rows), BF16),
        in_specs=[pl.BlockSpec(memory_space=pltpu.SMEM), VMEM],
        out_specs=VMEM,
        compiler_params=pltpu.CompilerParams(vmem_limit_bytes=16 * 2**20),
        cost_estimate=pl.CostEstimate(
            flops=n_q * qc * rows, bytes_accessed=4 * n_q * qc * rows, transcendentals=0
        ),
    )(lax.axis_index("zp").astype(jnp.int32)[None], query)

    part = call(
        functools.partial(attend_kernel, hd),
        jax.ShapeDtypeStruct((n_q, qc + 16, rows), BF16),
        2,
        4 * heads * n_q * rows * n_k * rows * hd,
        4 * n_q * qc * rows,
        exps=heads * n_q * rows * n_k * rows,
        limit=32,
        scratch=(
            pltpu.VMEM((n_k * rows, hd), BF16),
            pltpu.VMEM((hd + 16, n_k * rows), BF16),
            pltpu.VMEM((2, n_k * rows, 2 * rows), F32),
        ),
    )(query, kv)
    got = lax.all_to_all(part, ("y", "zp"), 0, 0, tiled=True)

    partial = call(
        functools.partial(mix_kernel, hd, n_tp),
        jax.ShapeDtypeStruct((n_tp, mine, d), BF16),
        2,
        2 * rows * qc * d,
        2 * d * (rows + qc),
        scratch=(pltpu.VMEM((qc, rows), F32),),
    )(got, w_out)
    got = lax.all_to_all(partial, TP, 0, 0, tiled=True)
    return got.astype(F32).sum(axis=0).astype(BF16)


def solution(mesh):
    finer = Mesh(mesh.devices.reshape(8, 2, 4, mesh.shape["tp"] // 2, 2), ALL)

    return jax.shard_map(
        body,
        mesh=finer,
        in_specs=(
            P(ALL, None),
            P(None, TP),
            P(None, TP),
            P(None, TP),
            P(TP, None),
            P(),
            P(),
        ),
        out_specs=P(ALL, None),
        check_vma=False,
    )
```

```python
import functools

import jax
import jax.numpy as jnp
from jax import lax
from jax.experimental import pallas as pl
from jax.experimental.pallas import tpu as pltpu
from jax.sharding import Mesh
from jax.sharding import PartitionSpec as P


F32, BF16 = jnp.float32, jnp.bfloat16
GRID_W = 64
SP = ("zq", "zp", "y")
TP = ("x", "c")
ALL = SP + TP
LOG2E = 1.4426950408889634
VMEM = pl.BlockSpec(memory_space=pltpu.VMEM)


def call(kernel, out, n_in, flops, byts, exps=0, limit=16, scratch=()):
    return pl.pallas_call(
        kernel,
        out_shape=out,
        in_specs=[VMEM] * n_in,
        out_specs=VMEM,
        scratch_shapes=list(scratch),
        compiler_params=pltpu.CompilerParams(vmem_limit_bytes=limit * 2**20),
        cost_estimate=pl.CostEstimate(flops=flops, bytes_accessed=byts, transcendentals=exps),
    )


def tables(gain, tab_ref):
    p = tab_ref.shape[1]
    gain = jnp.broadcast_to(gain, (tab_ref.shape[2], gain.shape[1])).T
    cosines, sines = [], []
    for half in range(2):
        cos, sin = tab_ref[2 * half], tab_ref[2 * half + 1]
        ga = gain[2 * half * p : (2 * half + 1) * p]
        gb = gain[(2 * half + 1) * p : (2 * half + 2) * p]
        cosines += [ga * cos, gb * cos]
        sines += [-gb * sin, ga * sin]
    return jnp.concatenate(cosines, axis=0), jnp.concatenate(sines, axis=0)


def turned(u, cos, sin):
    hd = u.shape[0]
    p = hd // 4
    swapped = jnp.concatenate([u[p : 2 * p], u[:p], u[3 * p :], u[2 * p : 3 * p]], axis=0)
    inv = lax.rsqrt(jnp.sum(u * u, axis=0, keepdims=True) * (1.0 / hd) + 1e-6)
    return (u * inv) * cos + (swapped * inv) * sin


NT = (((1,), (1,)), ((), ()))


def kv_kernel(copies, x_ref, wk_ref, wv_ref, gain_ref, tab_ref, out_ref):
    x = x_ref[...]
    k = lax.dot_general(wk_ref[...], x, NT, preferred_element_type=F32)
    v = lax.dot_general(wv_ref[...], x, NT, preferred_element_type=F32)
    kt = turned(k.astype(BF16).astype(F32), *tables(gain_ref[1:2], tab_ref)).astype(BF16)
    both = jnp.concatenate([kt, v.astype(BF16)], axis=0)
    for i in range(copies):
        out_ref[i] = both


def q_kernel(x_ref, w_ref, gain_ref, tab_ref, out_ref):
    q = jnp.dot(x_ref[...], w_ref[...], preferred_element_type=F32)
    qt = q.astype(BF16).astype(F32).T
    hd = gain_ref.shape[1]
    both = tables(gain_ref[0:1], tab_ref)
    for h in range(qt.shape[0] // hd):
        rows = slice(h * hd, (h + 1) * hd)
        out_ref[rows] = turned(qt[rows], *both).astype(BF16)


def pair_kernel(hd, zp_ref, q_ref, out_ref):
    n_q, qc, rows = q_ref.shape
    for i in range(n_q // 2):
        for b in range(2):
            block = 2 * i + (zp_ref[0] + b) % 2
            for h in range(qc // hd):
                out_ref[i, h, :, b * rows : (b + 1) * rows] = q_ref[
                    block, h * hd : (h + 1) * hd, :
                ]


def attend_kernel(hd, q_ref, kv_ref, out_ref, k_ref, v_ref, s_ref):
    n_pair, heads, _, rows = q_ref.shape
    rows //= 2
    n_k = kv_ref.shape[0]
    n_keys = n_k * rows
    step = n_keys // 2
    scale = hd**-0.5 * LOG2E
    for j in range(n_k):
        k_ref[j * rows : (j + 1) * rows, :] = kv_ref[j, :hd, :].astype(F32).T.astype(BF16)
        v_ref[16:, j * rows : (j + 1) * rows] = kv_ref[j, hd:, :]
    v_ref[:16, :] = jnp.ones((16, n_keys), BF16)

    def score(i, h, slot):
        top = None
        for c in range(0, n_keys, step):
            s = jnp.dot(k_ref[c : c + step, :], q_ref[i, h], preferred_element_type=F32)
            s_ref[slot, c : c + step] = s
            part = jnp.max(s.reshape(step // 8, 8, 2 * rows), axis=0)
            top = part if top is None else jnp.maximum(top, part)
        return (jnp.max(top, axis=0, keepdims=True) * scale).astype(BF16).astype(F32)

    left = lax.broadcasted_iota(jnp.int32, (1, rows), 1) < rows // 2

    def halves(a, b):
        return (
            jnp.where(left, a, pltpu.roll(b, rows // 2, 1)),
            jnp.where(left, pltpu.roll(a, rows // 2, 1), b),
        )

    def pair(i, top):
        outs, tops, sums = [], [], []
        for h in range(heads):
            if h + 1 < heads:
                later = score(i, h + 1, (h + 1) % 2)
            else:
                later = score(jnp.minimum(i + 1, n_pair - 1), 0, 0)
            o = 0.0
            for c in range(0, n_keys, step):
                p = jnp.exp2(s_ref[h % 2, c : c + step] * scale - top).astype(BF16)
                o += jnp.dot(v_ref[:, c : c + step], p, preferred_element_type=F32)
            outs.append(o[16:])
            sums.append(o[:1])
            tops.append(top)
            top = later
        total = jnp.concatenate(sums, axis=0)
        hi = total.astype(BF16).astype(F32)
        lo = total - hi
        tops = jnp.concatenate(tops, axis=0)
        n = heads // 2
        for b in range(2):
            lanes = slice(b * rows, (b + 1) * rows)
            for h in range(n):
                for c, part in enumerate(halves(outs[h][:, lanes], outs[h + n][:, lanes])):
                    out_ref[4 * i + 2 * b + c, h * hd : (h + 1) * hd, :] = part.astype(BF16)
            stats = [halves(r[:n, lanes], r[n:, lanes]) for r in (tops, hi, lo)]
            for c in range(2):
                both = [r[c] for r in stats] + [jnp.zeros((16 - 3 * n, rows), F32)]
                out_ref[4 * i + 2 * b + c, n * hd :, :] = jnp.concatenate(both, axis=0).astype(BF16)
        return top

    lax.fori_loop(0, n_pair, pair, score(0, 0, 0))


def mix_kernel(hd, core_ref, got_ref, own_ref, other_ref, out_ref):
    parts = got_ref.shape[0] // 2
    rows = got_ref.shape[2]
    n = own_ref.shape[0] // hd // 2
    far, mine, _ = out_ref.shape

    def mixed(core):
        st = [got_ref[2 * i + core, n * hd :, :].astype(F32) for i in range(parts)]
        top = functools.reduce(jnp.maximum, [s[:n] for s in st])
        factor = [jnp.exp2(s[:n] - top) for s in st]
        total = functools.reduce(
            jnp.add, [f * (s[n : 2 * n] + s[2 * n : 3 * n]) for f, s in zip(factor, st)]
        )
        heads = []
        for h in range(n):
            acc = 0.0
            for i in range(parts):
                acc += got_ref[2 * i + core, h * hd : (h + 1) * hd, :].astype(F32) * factor[i][h : h + 1]
            heads.append(acc / total[h : h + 1])
        turned_round = jnp.concatenate(heads, axis=0).T
        half = rows // 2
        return jnp.concatenate([turned_round[:half], turned_round[half:]], axis=1).astype(BF16)

    core = core_ref[0]
    out = jnp.dot(mixed(core), own_ref[...], preferred_element_type=F32)
    out += jnp.dot(mixed(1 - core), other_ref[...], preferred_element_type=F32)
    for x in range(far):
        out_ref[x] = out[x * mine : (x + 1) * mine].astype(BF16)


def body(tokens_in, w_query, w_key, w_value, w_out, q_gain, k_gain):
    hd = q_gain.shape[0]
    qc = w_query.shape[1]
    mine, d = tokens_in.shape
    n_tp = lax.axis_size(TP)
    rows = mine * n_tp
    n_k = lax.axis_size("zq")
    n_q = lax.axis_size(("zp", "y"))
    heads = qc // hd

    n_x, n_c = lax.axis_size("x"), lax.axis_size("c")
    lane = jnp.arange(rows, dtype=jnp.int32)
    core_of, x_of, row_of = lane // (n_x * mine), lane // mine % n_x, lane % mine
    position = lax.axis_index(SP) * rows + (x_of * n_c + core_of) * mine + row_of
    pairs = hd // 4
    freq = 10000.0 ** (-jnp.arange(pairs, dtype=F32) / pairs)
    grid = jnp.stack([position // GRID_W, position % GRID_W]).astype(F32)
    angle = grid[:, None, :] * freq[None, :, None]
    tab = jnp.stack([jnp.cos(angle), jnp.sin(angle)], axis=1).reshape(4, pairs, rows)
    gains = jnp.stack([q_gain, k_gain])
    tokens_in, tab, gains = lax.optimization_barrier((tokens_in, tab, gains))
    sent = jnp.broadcast_to(tokens_in[None], (lax.axis_size("x"), mine, d))
    tokens = lax.all_to_all(sent, "x", 0, 0, tiled=True)
    tokens = lax.all_gather(tokens, "c", axis=0).reshape(rows, d)

    query = call(
        q_kernel,
        jax.ShapeDtypeStruct((qc, rows), BF16),
        4,
        2 * rows * d * qc,
        2 * d * (rows + qc),
    )(tokens, w_query, gains, tab)
    other = lax.ppermute(query, "zp", [(0, 1), (1, 0)])
    kv = call(
        functools.partial(kv_kernel, n_k),
        jax.ShapeDtypeStruct((n_k, 2 * hd, rows), BF16),
        5,
        2 * rows * d * 2 * hd,
        2 * d * (rows + 2 * hd),
    )(tokens, w_key.T, w_value.T, gains, tab)
    kv = lax.all_to_all(kv, "zq", 0, 0, tiled=True)
    w_other = lax.ppermute(w_out, "c", [(0, 1), (1, 0)])
    query = lax.all_gather(jnp.stack([query, other]), "y", axis=0, tiled=True)
    query = pl.pallas_call(
        functools.partial(pair_kernel, hd),
        out_shape=jax.ShapeDtypeStruct((n_q // 2, heads, hd, 2 * rows), BF16),
        in_specs=[pl.BlockSpec(memory_space=pltpu.SMEM), VMEM],
        out_specs=VMEM,
        compiler_params=pltpu.CompilerParams(vmem_limit_bytes=16 * 2**20),
        cost_estimate=pl.CostEstimate(
            flops=n_q * qc * rows, bytes_accessed=4 * n_q * qc * rows, transcendentals=0
        ),
    )(lax.axis_index("zp").astype(jnp.int32)[None], query)

    core = lax.axis_index("c").astype(jnp.int32)[None]
    query, w_other, core = lax.optimization_barrier((query, w_other, core))
    part = call(
        functools.partial(attend_kernel, hd),
        jax.ShapeDtypeStruct((2 * n_q, qc // 2 + 16, rows), BF16),
        2,
        4 * heads * n_q * rows * n_k * rows * hd,
        4 * n_q * qc * rows,
        exps=heads * n_q * rows * n_k * rows,
        limit=32,
        scratch=(
            pltpu.VMEM((n_k * rows, hd), BF16),
            pltpu.VMEM((hd + 16, n_k * rows), BF16),
            pltpu.VMEM((2, n_k * rows, 2 * rows), F32),
        ),
    )(query, kv)
    got = lax.all_to_all(part, ("y", "zp", "c"), 0, 0, tiled=True)

    partial = pl.pallas_call(
        functools.partial(mix_kernel, hd),
        out_shape=jax.ShapeDtypeStruct((n_x, mine, d), BF16),
        in_specs=[pl.BlockSpec(memory_space=pltpu.SMEM)] + [VMEM] * 3,
        out_specs=VMEM,
        compiler_params=pltpu.CompilerParams(vmem_limit_bytes=16 * 2**20),
        cost_estimate=pl.CostEstimate(
            flops=2 * rows * qc * d, bytes_accessed=4 * d * qc, transcendentals=0
        ),
    )(core, got, w_out, w_other)
    got = lax.all_to_all(partial, "x", 0, 0, tiled=True)
    return got.astype(F32).sum(axis=0).astype(BF16)


def solution(mesh):
    finer = Mesh(mesh.devices.reshape(8, 2, 4, mesh.shape["tp"] // 2, 2), ALL)

    return jax.shard_map(
        body,
        mesh=finer,
        in_specs=(
            P(ALL, None),
            P(None, TP),
            P(None, TP),
            P(None, TP),
            P(TP, None),
            P(),
            P(),
        ),
        out_specs=P(ALL, None),
        check_vma=False,
    )
```

```python
import functools

import jax
import jax.numpy as jnp
from jax import lax
from jax.experimental import pallas as pl
from jax.experimental.pallas import tpu as pltpu
from jax.sharding import Mesh
from jax.sharding import PartitionSpec as P


F32, BF16 = jnp.float32, jnp.bfloat16
GRID_W = 64
SP = ("zq", "zp", "y")
TP = ("x", "c")
ALL = SP + TP
LOG2E = 1.4426950408889634
X_LEAD, Y_LEAD, Z_LEAD = 2, 2, 5
VMEM = pl.BlockSpec(memory_space=pltpu.VMEM)


def call(kernel, out, n_in, flops, byts, exps=0, limit=16, scratch=()):
    return pl.pallas_call(
        kernel,
        out_shape=out,
        in_specs=[VMEM] * n_in,
        out_specs=VMEM,
        scratch_shapes=list(scratch),
        compiler_params=pltpu.CompilerParams(vmem_limit_bytes=limit * 2**20),
        cost_estimate=pl.CostEstimate(flops=flops, bytes_accessed=byts, transcendentals=exps),
    )


def tables(gain, tab_ref):
    p = tab_ref.shape[1]
    gain = jnp.broadcast_to(gain, (tab_ref.shape[2], gain.shape[1])).T
    cosines, sines = [], []
    for half in range(2):
        cos, sin = tab_ref[2 * half], tab_ref[2 * half + 1]
        ga = gain[2 * half * p : (2 * half + 1) * p]
        gb = gain[(2 * half + 1) * p : (2 * half + 2) * p]
        cosines += [ga * cos, gb * cos]
        sines += [-gb * sin, ga * sin]
    return jnp.concatenate(cosines, axis=0), jnp.concatenate(sines, axis=0)


def led_by(lead, n):
    return [[(lead + i) % n for i in range(n)]]


def turned(u, cos, sin):
    hd = u.shape[0]
    p = hd // 4
    swapped = jnp.concatenate([u[p : 2 * p], u[:p], u[3 * p :], u[2 * p : 3 * p]], axis=0)
    inv = lax.rsqrt(jnp.sum(u * u, axis=0, keepdims=True) * (1.0 / hd) + 1e-6)
    return (u * inv) * cos + (swapped * inv) * sin


NT = (((1,), (1,)), ((), ()))


def kv_kernel(copies, x_ref, wk_ref, wv_ref, gain_ref, tab_ref, out_ref):
    x = x_ref[...]
    k = lax.dot_general(wk_ref[...], x, NT, preferred_element_type=F32)
    v = lax.dot_general(wv_ref[...], x, NT, preferred_element_type=F32)
    kt = turned(k.astype(BF16).astype(F32), *tables(gain_ref[1:2], tab_ref)).astype(BF16)
    both = jnp.concatenate([kt, v.astype(BF16)], axis=0)
    for i in range(copies):
        out_ref[i] = both


def q_kernel(x_ref, w_ref, gain_ref, tab_ref, out_ref):
    q = jnp.dot(x_ref[...], w_ref[...], preferred_element_type=F32)
    qt = q.astype(BF16).astype(F32).T
    hd = gain_ref.shape[1]
    both = tables(gain_ref[0:1], tab_ref)
    for h in range(qt.shape[0] // hd):
        rows = slice(h * hd, (h + 1) * hd)
        out_ref[rows] = turned(qt[rows], *both).astype(BF16)


def pair_kernel(hd, zp_ref, q_ref, out_ref):
    n_q, qc, rows = q_ref.shape
    for i in range(n_q // 2):
        for b in range(2):
            block = 2 * i + (zp_ref[0] + b) % 2
            for h in range(qc // hd):
                out_ref[i, h, :, b * rows : (b + 1) * rows] = q_ref[
                    block, h * hd : (h + 1) * hd, :
                ]


def attend_kernel(hd, q_ref, kv_ref, out_ref, k_ref, v_ref, s_ref):
    n_pair, heads, _, rows = q_ref.shape
    rows //= 2
    n_k = kv_ref.shape[0]
    n_keys = n_k * rows
    step = n_keys // 2
    scale = hd**-0.5 * LOG2E
    for j in range(n_k):
        k_ref[j * rows : (j + 1) * rows, :] = kv_ref[j, :hd, :].astype(F32).T.astype(BF16)
        v_ref[16:, j * rows : (j + 1) * rows] = kv_ref[j, hd:, :]
    v_ref[:16, :] = jnp.ones((16, n_keys), BF16)

    def score(i, h, slot):
        top = None
        for c in range(0, n_keys, step):
            s = jnp.dot(k_ref[c : c + step, :], q_ref[i, h], preferred_element_type=F32)
            s_ref[slot, c : c + step] = s
            part = jnp.max(s.reshape(step // 8, 8, 2 * rows), axis=0)
            top = part if top is None else jnp.maximum(top, part)
        return (jnp.max(top, axis=0, keepdims=True) * scale).astype(BF16).astype(F32)

    left = lax.broadcasted_iota(jnp.int32, (1, rows), 1) < rows // 2

    def halves(a, b):
        return (
            jnp.where(left, a, pltpu.roll(b, rows // 2, 1)),
            jnp.where(left, pltpu.roll(a, rows // 2, 1), b),
        )

    def pair(i, top):
        outs, tops, sums = [], [], []
        for h in range(heads):
            if h + 1 < heads:
                later = score(i, h + 1, (h + 1) % 2)
            else:
                later = score(jnp.minimum(i + 1, n_pair - 1), 0, 0)
            o = 0.0
            for c in range(0, n_keys, step):
                p = jnp.exp2(s_ref[h % 2, c : c + step] * scale - top).astype(BF16)
                o += jnp.dot(v_ref[:, c : c + step], p, preferred_element_type=F32)
            outs.append(o[16:])
            sums.append(o[:1])
            tops.append(top)
            top = later
        total = jnp.concatenate(sums, axis=0)
        hi = total.astype(BF16).astype(F32)
        lo = total - hi
        tops = jnp.concatenate(tops, axis=0)
        n = heads // 2
        for b in range(2):
            lanes = slice(b * rows, (b + 1) * rows)
            for h in range(n):
                for c, part in enumerate(halves(outs[h][:, lanes], outs[h + n][:, lanes])):
                    out_ref[4 * i + 2 * b + c, h * hd : (h + 1) * hd, :] = part.astype(BF16)
            stats = [halves(r[:n, lanes], r[n:, lanes]) for r in (tops, hi, lo)]
            for c in range(2):
                both = [r[c] for r in stats] + [jnp.zeros((16 - 3 * n, rows), F32)]
                out_ref[4 * i + 2 * b + c, n * hd :, :] = jnp.concatenate(both, axis=0).astype(BF16)
        return top

    lax.fori_loop(0, n_pair, pair, score(0, 0, 0))


def mix_kernel(hd, core_ref, got_ref, own_ref, other_ref, out_ref):
    parts = got_ref.shape[0] // 2
    rows = got_ref.shape[2]
    n = own_ref.shape[0] // hd // 2
    far, mine, _ = out_ref.shape

    def mixed(core):
        st = [got_ref[2 * i + core, n * hd :, :].astype(F32) for i in range(parts)]
        top = functools.reduce(jnp.maximum, [s[:n] for s in st])
        factor = [jnp.exp2(s[:n] - top) for s in st]
        total = functools.reduce(
            jnp.add, [f * (s[n : 2 * n] + s[2 * n : 3 * n]) for f, s in zip(factor, st)]
        )
        heads = []
        for h in range(n):
            acc = 0.0
            for i in range(parts):
                acc += got_ref[2 * i + core, h * hd : (h + 1) * hd, :].astype(F32) * factor[i][h : h + 1]
            heads.append(acc / total[h : h + 1])
        turned_round = jnp.concatenate(heads, axis=0).T
        half = rows // 2
        return jnp.concatenate([turned_round[:half], turned_round[half:]], axis=1).astype(BF16)

    core = core_ref[0]
    out = jnp.dot(mixed(core), own_ref[...], preferred_element_type=F32)
    out += jnp.dot(mixed(1 - core), other_ref[...], preferred_element_type=F32)
    for x in range(far):
        out_ref[x] = out[x * mine : (x + 1) * mine].astype(BF16)


def body(tokens_in, w_query, w_key, w_value, w_out, q_gain, k_gain):
    hd = q_gain.shape[0]
    qc = w_query.shape[1]
    mine, d = tokens_in.shape
    n_tp = lax.axis_size(TP)
    rows = mine * n_tp
    n_k = lax.axis_size("zq")
    n_q = lax.axis_size(("zp", "y"))
    heads = qc // hd

    n_x, n_c = lax.axis_size("x"), lax.axis_size("c")
    lane = jnp.arange(rows, dtype=jnp.int32)
    core_of, x_of, row_of = lane // (n_x * mine), (lane // mine + X_LEAD) % n_x, lane % mine
    position = lax.axis_index(SP) * rows + (x_of * n_c + core_of) * mine + row_of
    pairs = hd // 4
    freq = 10000.0 ** (-jnp.arange(pairs, dtype=F32) / pairs)
    grid = jnp.stack([position // GRID_W, position % GRID_W]).astype(F32)
    angle = grid[:, None, :] * freq[None, :, None]
    tab = jnp.stack([jnp.cos(angle), jnp.sin(angle)], axis=1).reshape(4, pairs, rows)
    gains = jnp.stack([q_gain, k_gain])
    tokens_in, tab, gains = lax.optimization_barrier((tokens_in, tab, gains))
    sent = jnp.broadcast_to(tokens_in[None], (lax.axis_size("x"), mine, d))
    tokens = lax.all_to_all(sent, "x", 0, 0, tiled=True, axis_index_groups=led_by(X_LEAD, n_x))
    tokens = lax.all_gather(tokens, "c", axis=0).reshape(rows, d)

    query = call(
        q_kernel,
        jax.ShapeDtypeStruct((qc, rows), BF16),
        4,
        2 * rows * d * qc,
        2 * d * (rows + qc),
    )(tokens, w_query, gains, tab)
    other = lax.ppermute(query, "zp", [(0, 1), (1, 0)])
    kv = call(
        functools.partial(kv_kernel, n_k),
        jax.ShapeDtypeStruct((n_k, 2 * hd, rows), BF16),
        5,
        2 * rows * d * 2 * hd,
        2 * d * (rows + 2 * hd),
    )(tokens, w_key.T, w_value.T, gains, tab)
    kv = lax.all_to_all(kv, "zq", 0, 0, tiled=True, axis_index_groups=led_by(Z_LEAD, n_k))
    w_other = lax.ppermute(w_out, "c", [(0, 1), (1, 0)])
    query = lax.all_gather(
        jnp.stack([query, other]), "y", axis=0, tiled=True, axis_index_groups=led_by(Y_LEAD, n_q // 2)
    )
    query = pl.pallas_call(
        functools.partial(pair_kernel, hd),
        out_shape=jax.ShapeDtypeStruct((n_q // 2, heads, hd, 2 * rows), BF16),
        in_specs=[pl.BlockSpec(memory_space=pltpu.SMEM), VMEM],
        out_specs=VMEM,
        compiler_params=pltpu.CompilerParams(vmem_limit_bytes=16 * 2**20),
        cost_estimate=pl.CostEstimate(
            flops=n_q * qc * rows, bytes_accessed=4 * n_q * qc * rows, transcendentals=0
        ),
    )(lax.axis_index("zp").astype(jnp.int32)[None], query)

    core = lax.axis_index("c").astype(jnp.int32)[None]
    query, w_other, core = lax.optimization_barrier((query, w_other, core))
    part = call(
        functools.partial(attend_kernel, hd),
        jax.ShapeDtypeStruct((2 * n_q, qc // 2 + 16, rows), BF16),
        2,
        4 * heads * n_q * rows * n_k * rows * hd,
        4 * n_q * qc * rows,
        exps=heads * n_q * rows * n_k * rows,
        limit=32,
        scratch=(
            pltpu.VMEM((n_k * rows, hd), BF16),
            pltpu.VMEM((hd + 16, n_k * rows), BF16),
            pltpu.VMEM((2, n_k * rows, 2 * rows), F32),
        ),
    )(query, kv)
    got = lax.all_to_all(
        part, ("y", "zp", "c"), 0, 0, tiled=True, axis_index_groups=led_by(Y_LEAD * 4, 2 * n_q)
    )

    partial = pl.pallas_call(
        functools.partial(mix_kernel, hd),
        out_shape=jax.ShapeDtypeStruct((n_x, mine, d), BF16),
        in_specs=[pl.BlockSpec(memory_space=pltpu.SMEM)] + [VMEM] * 3,
        out_specs=VMEM,
        compiler_params=pltpu.CompilerParams(vmem_limit_bytes=16 * 2**20),
        cost_estimate=pl.CostEstimate(
            flops=2 * rows * qc * d, bytes_accessed=4 * d * qc, transcendentals=0
        ),
    )(core, got, w_out, w_other)
    got = lax.all_to_all(partial, "x", 0, 0, tiled=True, axis_index_groups=led_by(X_LEAD, n_x))
    return got.astype(F32).sum(axis=0).astype(BF16)


def solution(mesh):
    finer = Mesh(mesh.devices.reshape(8, 2, 4, mesh.shape["tp"] // 2, 2), ALL)

    return jax.shard_map(
        body,
        mesh=finer,
        in_specs=(
            P(ALL, None),
            P(None, TP),
            P(None, TP),
            P(None, TP),
            P(TP, None),
            P(),
            P(),
        ),
        out_specs=P(ALL, None),
        check_vma=False,
    )
```

```python
import functools

import jax
import jax.numpy as jnp
from jax import lax
from jax.experimental import pallas as pl
from jax.experimental.pallas import tpu as pltpu
from jax.sharding import Mesh
from jax.sharding import PartitionSpec as P


F32, BF16 = jnp.float32, jnp.bfloat16
GRID_W = 64
SP = ("zq", "zp", "y")
TP = ("x", "c")
ALL = SP + TP
LOG2E = 1.4426950408889634
X_LEAD, Y_LEAD, Z_LEAD = 2, 2, 5
VMEM = pl.BlockSpec(memory_space=pltpu.VMEM)


def call(kernel, out, n_in, flops, byts, exps=0, limit=16, scratch=()):
    return pl.pallas_call(
        kernel,
        out_shape=out,
        in_specs=[VMEM] * n_in,
        out_specs=VMEM,
        scratch_shapes=list(scratch),
        compiler_params=pltpu.CompilerParams(vmem_limit_bytes=limit * 2**20),
        cost_estimate=pl.CostEstimate(flops=flops, bytes_accessed=byts, transcendentals=exps),
    )


def tables(gain, tab_ref):
    p = tab_ref.shape[1]
    gain = jnp.broadcast_to(gain, (tab_ref.shape[2], gain.shape[1])).T
    cosines, sines = [], []
    for half in range(2):
        cos, sin = tab_ref[2 * half], tab_ref[2 * half + 1]
        ga = gain[2 * half * p : (2 * half + 1) * p]
        gb = gain[(2 * half + 1) * p : (2 * half + 2) * p]
        cosines += [ga * cos, gb * cos]
        sines += [-gb * sin, ga * sin]
    return jnp.concatenate(cosines, axis=0), jnp.concatenate(sines, axis=0)


def led_by(lead, n):
    return [[(lead + i) % n for i in range(n)]]


def turned(u, cos, sin):
    hd = u.shape[0]
    p = hd // 4
    swapped = jnp.concatenate([u[p : 2 * p], u[:p], u[3 * p :], u[2 * p : 3 * p]], axis=0)
    inv = lax.rsqrt(jnp.sum(u * u, axis=0, keepdims=True) * (1.0 / hd) + 1e-6)
    return (u * inv) * cos + (swapped * inv) * sin


NT = (((1,), (1,)), ((), ()))


def kv_kernel(copies, x_ref, wk_ref, wv_ref, gain_ref, tab_ref, out_ref):
    x = x_ref[...]
    k = lax.dot_general(wk_ref[...], x, NT, preferred_element_type=F32)
    v = lax.dot_general(wv_ref[...], x, NT, preferred_element_type=F32)
    kt = turned(k.astype(BF16).astype(F32), *tables(gain_ref[1:2], tab_ref)).astype(BF16)
    both = jnp.concatenate([kt, v.astype(BF16)], axis=0)
    for i in range(copies):
        out_ref[i] = both


def q_kernel(x_ref, w_ref, gain_ref, tab_ref, out_ref):
    q = jnp.dot(x_ref[...], w_ref[...], preferred_element_type=F32)
    qt = q.astype(BF16).astype(F32).T
    hd = gain_ref.shape[1]
    both = tables(gain_ref[0:1], tab_ref)
    for h in range(qt.shape[0] // hd):
        rows = slice(h * hd, (h + 1) * hd)
        out_ref[rows] = turned(qt[rows], *both).astype(BF16)


def attend_kernel(hd, zp_ref, q_ref, kv_ref, out_ref, k_ref, v_ref, s_ref):
    n_q, qc, rows = q_ref.shape
    n_pair, heads = n_q // 2, qc // hd
    n_k = kv_ref.shape[0]
    n_keys = n_k * rows
    spots = zp_ref[0], 1 - zp_ref[0]
    step = n_keys // 2
    scale = hd**-0.5 * LOG2E
    for j in range(n_k):
        k_ref[j * rows : (j + 1) * rows, :] = kv_ref[j, :hd, :].astype(F32).T.astype(BF16)
        v_ref[16:, j * rows : (j + 1) * rows] = kv_ref[j, hd:, :]
    v_ref[:16, :] = jnp.ones((16, n_keys), BF16)

    def score(i, h, slot):
        top = None
        q = jnp.concatenate(
            [q_ref[2 * i + b, h * hd : (h + 1) * hd, :] for b in range(2)], axis=1
        )
        for c in range(0, n_keys, step):
            s = jnp.dot(k_ref[c : c + step, :], q, preferred_element_type=F32)
            s_ref[slot, c : c + step] = s
            part = jnp.max(s.reshape(step // 8, 8, 2 * rows), axis=0)
            top = part if top is None else jnp.maximum(top, part)
        return (jnp.max(top, axis=0, keepdims=True) * scale).astype(BF16).astype(F32)

    def pair(i, top):
        tops, sums = [], []
        for h in range(heads):
            if h + 1 < heads:
                later = score(i, h + 1, (h + 1) % 2)
            else:
                later = score(jnp.minimum(i + 1, n_pair - 1), 0, 0)
            o = 0.0
            for c in range(0, n_keys, step):
                p = jnp.exp2(s_ref[h % 2, c : c + step] * scale - top).astype(BF16)
                o += jnp.dot(v_ref[:, c : c + step], p, preferred_element_type=F32)
            tops.append(top)
            sums.append(o[:1])
            for b in range(2):
                out_ref[2 * i + spots[b], h * hd : (h + 1) * hd, :] = o[
                    16:, b * rows : (b + 1) * rows
                ].astype(BF16)
            top = later
        total = jnp.concatenate(sums, axis=0)
        hi = total.astype(BF16).astype(F32)
        stats = jnp.concatenate(tops + [hi, total - hi, jnp.zeros_like(total)], axis=0).astype(BF16)
        for b in range(2):
            out_ref[2 * i + spots[b], qc:, :] = stats[:, b * rows : (b + 1) * rows]
        return top

    lax.fori_loop(0, n_pair, pair, score(0, 0, 0))


def mix_kernel(hd, n_tp, got_ref, w_ref, out_ref, mixed_ref):
    parts, _, rows = got_ref.shape
    qc = w_ref.shape[0]
    heads = qc // hd
    st = [got_ref[i, qc:, :].astype(F32) for i in range(parts)]
    top = functools.reduce(jnp.maximum, [s[:heads] for s in st])
    factor = [jnp.exp2(s[:heads] - top) for s in st]
    total = functools.reduce(
        jnp.add,
        [f * (s[heads : 2 * heads] + s[2 * heads : 3 * heads]) for f, s in zip(factor, st)],
    )
    for h in range(heads):
        acc = 0.0
        for i in range(parts):
            acc += got_ref[i, h * hd : (h + 1) * hd, :].astype(F32) * factor[i][h : h + 1]
        mixed_ref[h * hd : (h + 1) * hd, :] = acc / total[h : h + 1]
    mixed = mixed_ref[...].T.astype(BF16)
    out = jnp.dot(mixed, w_ref[...], preferred_element_type=F32).astype(BF16)
    each = rows // n_tp
    for t in range(n_tp):
        at = t % 2 * (n_tp // 2) + t // 2
        out_ref[t] = out[at * each : (at + 1) * each]


def body(tokens_in, w_query, w_key, w_value, w_out, q_gain, k_gain):
    hd = q_gain.shape[0]
    qc = w_query.shape[1]
    mine, d = tokens_in.shape
    n_tp = lax.axis_size(TP)
    rows = mine * n_tp
    n_k = lax.axis_size("zq")
    n_q = lax.axis_size(("zp", "y"))
    heads = qc // hd

    n_x, n_c = lax.axis_size("x"), lax.axis_size("c")
    lane = jnp.arange(rows, dtype=jnp.int32)
    core_of, x_of, row_of = lane // (n_x * mine), (lane // mine + X_LEAD) % n_x, lane % mine
    position = lax.axis_index(SP) * rows + (x_of * n_c + core_of) * mine + row_of
    pairs = hd // 4
    freq = 10000.0 ** (-jnp.arange(pairs, dtype=F32) / pairs)
    grid = jnp.stack([position // GRID_W, position % GRID_W]).astype(F32)
    angle = grid[:, None, :] * freq[None, :, None]
    tab = jnp.stack([jnp.cos(angle), jnp.sin(angle)], axis=1).reshape(4, pairs, rows)
    gains = jnp.stack([q_gain, k_gain])
    tokens_in, tab, gains = lax.optimization_barrier((tokens_in, tab, gains))
    sent = jnp.broadcast_to(tokens_in[None], (lax.axis_size("x"), mine, d))
    tokens = lax.all_to_all(sent, "x", 0, 0, tiled=True, axis_index_groups=led_by(X_LEAD, n_x))
    tokens = lax.all_gather(tokens, "c", axis=0).reshape(rows, d)

    query = call(
        q_kernel,
        jax.ShapeDtypeStruct((qc, rows), BF16),
        4,
        2 * rows * d * qc,
        2 * d * (rows + qc),
    )(tokens, w_query, gains, tab)
    other = lax.ppermute(query, "zp", [(0, 1), (1, 0)])
    kv = call(
        functools.partial(kv_kernel, n_k),
        jax.ShapeDtypeStruct((n_k, 2 * hd, rows), BF16),
        5,
        2 * rows * d * 2 * hd,
        2 * d * (rows + 2 * hd),
    )(tokens, w_key.T, w_value.T, gains, tab)
    kv = lax.all_to_all(kv, "zq", 0, 0, tiled=True, axis_index_groups=led_by(Z_LEAD, n_k))
    query = lax.all_gather(
        jnp.stack([query, other]), "y", axis=0, tiled=True, axis_index_groups=led_by(Y_LEAD, n_q // 2)
    )
    part = pl.pallas_call(
        functools.partial(attend_kernel, hd),
        out_shape=jax.ShapeDtypeStruct((n_q, qc + 16, rows), BF16),
        in_specs=[pl.BlockSpec(memory_space=pltpu.SMEM), VMEM, VMEM],
        out_specs=VMEM,
        scratch_shapes=[
            pltpu.VMEM((n_k * rows, hd), BF16),
            pltpu.VMEM((hd + 16, n_k * rows), BF16),
            pltpu.VMEM((2, n_k * rows, 2 * rows), F32),
        ],
        compiler_params=pltpu.CompilerParams(vmem_limit_bytes=32 * 2**20),
        cost_estimate=pl.CostEstimate(
            flops=4 * heads * n_q * rows * n_k * rows * hd,
            bytes_accessed=4 * n_q * qc * rows,
            transcendentals=heads * n_q * rows * n_k * rows,
        ),
    )(lax.axis_index("zp").astype(jnp.int32)[None], query, kv)
    got = lax.all_to_all(
        part, ("y", "zp"), 0, 0, tiled=True, axis_index_groups=led_by(Y_LEAD * 2, n_q)
    )

    partial = call(
        functools.partial(mix_kernel, hd, n_tp),
        jax.ShapeDtypeStruct((n_tp, mine, d), BF16),
        2,
        2 * rows * qc * d,
        2 * d * (rows + qc),
        scratch=(pltpu.VMEM((qc, rows), F32),),
    )(got, w_out)
    got = lax.all_to_all(
        partial, TP, 0, 0, tiled=True, axis_index_groups=led_by(X_LEAD * n_c, n_tp)
    )
    return got.astype(F32).sum(axis=0).astype(BF16)


def solution(mesh):
    finer = Mesh(mesh.devices.reshape(8, 2, 4, mesh.shape["tp"] // 2, 2), ALL)

    return jax.shard_map(
        body,
        mesh=finer,
        in_specs=(
            P(ALL, None),
            P(None, TP),
            P(None, TP),
            P(None, TP),
            P(TP, None),
            P(),
            P(),
        ),
        out_specs=P(ALL, None),
        check_vma=False,
    )
```

```python
import functools

import jax
import jax.numpy as jnp
from jax import lax
from jax.experimental import pallas as pl
from jax.experimental.pallas import tpu as pltpu
from jax.sharding import Mesh
from jax.sharding import PartitionSpec as P


F32, BF16 = jnp.float32, jnp.bfloat16
GRID_W = 64
SP = ("zq", "zp", "y")
TP = ("x", "c")
ALL = SP + TP
LOG2E = 1.4426950408889634
C_LEAD, OUT_LEAD, X_LEAD, Y_LEAD, Z_LEAD = 1, 5, 2, 2, 5
VMEM = pl.BlockSpec(memory_space=pltpu.VMEM)


def call(kernel, out, n_in, flops, byts, exps=0, limit=16, scratch=()):
    return pl.pallas_call(
        kernel,
        out_shape=out,
        in_specs=[VMEM] * n_in,
        out_specs=VMEM,
        scratch_shapes=list(scratch),
        compiler_params=pltpu.CompilerParams(vmem_limit_bytes=limit * 2**20),
        cost_estimate=pl.CostEstimate(flops=flops, bytes_accessed=byts, transcendentals=exps),
    )


def tables(gain, tab_ref):
    p = tab_ref.shape[1]
    gain = jnp.broadcast_to(gain, (tab_ref.shape[2], gain.shape[1])).T
    cosines, sines = [], []
    for half in range(2):
        cos, sin = tab_ref[2 * half], tab_ref[2 * half + 1]
        ga = gain[2 * half * p : (2 * half + 1) * p]
        gb = gain[(2 * half + 1) * p : (2 * half + 2) * p]
        cosines += [ga * cos, gb * cos]
        sines += [-gb * sin, ga * sin]
    return jnp.concatenate(cosines, axis=0), jnp.concatenate(sines, axis=0)


def led_by(lead, n):
    return [[(lead + i) % n for i in range(n)]]


def turned(u, cos, sin):
    hd = u.shape[0]
    p = hd // 4
    swapped = jnp.concatenate([u[p : 2 * p], u[:p], u[3 * p :], u[2 * p : 3 * p]], axis=0)
    inv = lax.rsqrt(jnp.sum(u * u, axis=0, keepdims=True) * (1.0 / hd) + 1e-6)
    return (u * inv) * cos + (swapped * inv) * sin


NT = (((1,), (1,)), ((), ()))


def kv_kernel(copies, x_ref, wk_ref, wv_ref, gain_ref, tab_ref, out_ref):
    x = x_ref[...]
    k = lax.dot_general(wk_ref[...], x, NT, preferred_element_type=F32)
    v = lax.dot_general(wv_ref[...], x, NT, preferred_element_type=F32)
    kt = turned(k.astype(BF16).astype(F32), *tables(gain_ref[1:2], tab_ref)).astype(BF16)
    both = jnp.concatenate([kt, v.astype(BF16)], axis=0)
    for i in range(copies):
        out_ref[i] = both


def q_kernel(x_ref, w_ref, gain_ref, tab_ref, out_ref):
    q = jnp.dot(x_ref[...], w_ref[...], preferred_element_type=F32)
    qt = q.astype(BF16).astype(F32).T
    hd = gain_ref.shape[1]
    both = tables(gain_ref[0:1], tab_ref)
    for h in range(qt.shape[0] // hd):
        rows = slice(h * hd, (h + 1) * hd)
        out_ref[rows] = turned(qt[rows], *both).astype(BF16)


def attend_kernel(hd, zp_ref, q_ref, kv_ref, out_ref, k_ref, v_ref, s_ref):
    n_q, qc, rows = q_ref.shape
    n_pair, heads = n_q // 2, qc // hd
    n_k = kv_ref.shape[0]
    n_keys = n_k * rows
    spots = zp_ref[0], 1 - zp_ref[0]
    step = n_keys // 2
    scale = hd**-0.5 * LOG2E
    for j in range(n_k):
        k_ref[j * rows : (j + 1) * rows, :] = kv_ref[j, :hd, :].astype(F32).T.astype(BF16)
        v_ref[16:, j * rows : (j + 1) * rows] = kv_ref[j, hd:, :]
    v_ref[:16, :] = jnp.ones((16, n_keys), BF16)

    def score(i, h, slot):
        top = None
        q = jnp.concatenate(
            [q_ref[2 * i + b, h * hd : (h + 1) * hd, :] for b in range(2)], axis=1
        )
        for c in range(0, n_keys, step):
            s = jnp.dot(k_ref[c : c + step, :], q, preferred_element_type=F32)
            s_ref[slot, c : c + step] = s
            part = jnp.max(s.reshape(step // 8, 8, 2 * rows), axis=0)
            top = part if top is None else jnp.maximum(top, part)
        return (jnp.max(top, axis=0, keepdims=True) * scale).astype(BF16).astype(F32)

    def pair(i, top):
        tops, sums = [], []
        for h in range(heads):
            if h + 1 < heads:
                later = score(i, h + 1, (h + 1) % 2)
            else:
                later = score(jnp.minimum(i + 1, n_pair - 1), 0, 0)
            o = 0.0
            for c in range(0, n_keys, step):
                p = jnp.exp2(s_ref[h % 2, c : c + step] * scale - top).astype(BF16)
                o += jnp.dot(v_ref[:, c : c + step], p, preferred_element_type=F32)
            tops.append(top)
            sums.append(o[:1])
            for b in range(2):
                out_ref[2 * i + spots[b], h * hd : (h + 1) * hd, :] = o[
                    16:, b * rows : (b + 1) * rows
                ].astype(BF16)
            top = later
        total = jnp.concatenate(sums, axis=0)
        hi = total.astype(BF16).astype(F32)
        stats = jnp.concatenate(tops + [hi, total - hi, jnp.zeros_like(total)], axis=0).astype(BF16)
        for b in range(2):
            out_ref[2 * i + spots[b], qc:, :] = stats[:, b * rows : (b + 1) * rows]
        return top

    lax.fori_loop(0, n_pair, pair, score(0, 0, 0))


def mix_kernel(hd, n_tp, got_ref, w_ref, out_ref, mixed_ref):
    parts, _, rows = got_ref.shape
    qc = w_ref.shape[0]
    heads = qc // hd
    st = [got_ref[i, qc:, :].astype(F32) for i in range(parts)]
    top = functools.reduce(jnp.maximum, [s[:heads] for s in st])
    factor = [jnp.exp2(s[:heads] - top) for s in st]
    total = functools.reduce(
        jnp.add,
        [f * (s[heads : 2 * heads] + s[2 * heads : 3 * heads]) for f, s in zip(factor, st)],
    )
    for h in range(heads):
        acc = 0.0
        for i in range(parts):
            acc += got_ref[i, h * hd : (h + 1) * hd, :].astype(F32) * factor[i][h : h + 1]
        mixed_ref[h * hd : (h + 1) * hd, :] = acc / total[h : h + 1]
    mixed = mixed_ref[...].T.astype(BF16)
    out = jnp.dot(mixed, w_ref[...], preferred_element_type=F32).astype(BF16)
    each = rows // n_tp
    for t in range(n_tp):
        to = (OUT_LEAD + t) % n_tp
        at = (to % 2 + C_LEAD) % 2 * (n_tp // 2) + (to // 2 - X_LEAD) % (n_tp // 2)
        out_ref[t] = out[at * each : (at + 1) * each]


def body(tokens_in, w_query, w_key, w_value, w_out, q_gain, k_gain):
    hd = q_gain.shape[0]
    qc = w_query.shape[1]
    mine, d = tokens_in.shape
    n_tp = lax.axis_size(TP)
    rows = mine * n_tp
    n_k = lax.axis_size("zq")
    n_q = lax.axis_size(("zp", "y"))
    heads = qc // hd

    n_x, n_c = lax.axis_size("x"), lax.axis_size("c")
    lane = jnp.arange(rows, dtype=jnp.int32)
    core_of, x_of, row_of = (lane // (n_x * mine) + C_LEAD) % n_c, (lane // mine + X_LEAD) % n_x, lane % mine
    position = lax.axis_index(SP) * rows + (x_of * n_c + core_of) * mine + row_of
    pairs = hd // 4
    freq = 10000.0 ** (-jnp.arange(pairs, dtype=F32) / pairs)
    grid = jnp.stack([position // GRID_W, position % GRID_W]).astype(F32)
    angle = grid[:, None, :] * freq[None, :, None]
    tab = jnp.stack([jnp.cos(angle), jnp.sin(angle)], axis=1).reshape(4, pairs, rows)
    gains = jnp.stack([q_gain, k_gain])
    tokens_in, tab, gains = lax.optimization_barrier((tokens_in, tab, gains))
    sent = jnp.broadcast_to(tokens_in[None], (lax.axis_size("x"), mine, d))
    tokens = lax.all_to_all(sent, "x", 0, 0, tiled=True, axis_index_groups=led_by(X_LEAD, n_x))
    tokens = lax.all_gather(tokens, "c", axis=0, axis_index_groups=led_by(C_LEAD, n_c)).reshape(rows, d)

    query = call(
        q_kernel,
        jax.ShapeDtypeStruct((qc, rows), BF16),
        4,
        2 * rows * d * qc,
        2 * d * (rows + qc),
    )(tokens, w_query, gains, tab)
    other = lax.ppermute(query, "zp", [(0, 1), (1, 0)])
    kv = call(
        functools.partial(kv_kernel, n_k),
        jax.ShapeDtypeStruct((n_k, 2 * hd, rows), BF16),
        5,
        2 * rows * d * 2 * hd,
        2 * d * (rows + 2 * hd),
    )(tokens, w_key.T, w_value.T, gains, tab)
    kv = lax.all_to_all(kv, "zq", 0, 0, tiled=True, axis_index_groups=led_by(Z_LEAD, n_k))
    query = lax.all_gather(
        jnp.stack([query, other]), "y", axis=0, tiled=True, axis_index_groups=led_by(Y_LEAD, n_q // 2)
    )
    part = pl.pallas_call(
        functools.partial(attend_kernel, hd),
        out_shape=jax.ShapeDtypeStruct((n_q, qc + 16, rows), BF16),
        in_specs=[pl.BlockSpec(memory_space=pltpu.SMEM), VMEM, VMEM],
        out_specs=VMEM,
        scratch_shapes=[
            pltpu.VMEM((n_k * rows, hd), BF16),
            pltpu.VMEM((hd + 16, n_k * rows), BF16),
            pltpu.VMEM((2, n_k * rows, 2 * rows), F32),
        ],
        compiler_params=pltpu.CompilerParams(vmem_limit_bytes=32 * 2**20),
        cost_estimate=pl.CostEstimate(
            flops=4 * heads * n_q * rows * n_k * rows * hd,
            bytes_accessed=4 * n_q * qc * rows,
            transcendentals=heads * n_q * rows * n_k * rows,
        ),
    )(lax.axis_index("zp").astype(jnp.int32)[None], query, kv)
    got = lax.all_to_all(
        part, ("y", "zp"), 0, 0, tiled=True, axis_index_groups=led_by(Y_LEAD * 2, n_q)
    )

    partial = call(
        functools.partial(mix_kernel, hd, n_tp),
        jax.ShapeDtypeStruct((n_tp, mine, d), BF16),
        2,
        2 * rows * qc * d,
        2 * d * (rows + qc),
        scratch=(pltpu.VMEM((qc, rows), F32),),
    )(got, w_out)
    got = lax.all_to_all(
        partial, TP, 0, 0, tiled=True, axis_index_groups=led_by(OUT_LEAD, n_tp)
    )
    return got.astype(F32).sum(axis=0).astype(BF16)


def solution(mesh):
    finer = Mesh(mesh.devices.reshape(8, 2, 4, mesh.shape["tp"] // 2, 2), ALL)

    return jax.shard_map(
        body,
        mesh=finer,
        in_specs=(
            P(ALL, None),
            P(None, TP),
            P(None, TP),
            P(None, TP),
            P(TP, None),
            P(),
            P(),
        ),
        out_specs=P(ALL, None),
        check_vma=False,
    )
```

```python
import functools

import jax
import jax.numpy as jnp
from jax import lax
from jax.experimental import pallas as pl
from jax.experimental.pallas import tpu as pltpu
from jax.sharding import Mesh
from jax.sharding import PartitionSpec as P


F32, BF16 = jnp.float32, jnp.bfloat16
GRID_W = 64
SP = ("zq", "zp", "y")
TP = ("x", "c")
ALL = SP + TP
LOG2E = 1.4426950408889634
C_LEAD, OUT_LEAD, X_LEAD, Z_LEAD = 1, 5, 2, 5
Y_ORDER = 2, 1, 0, 3
VMEM = pl.BlockSpec(memory_space=pltpu.VMEM)


def call(kernel, out, n_in, flops, byts, exps=0, limit=16, scratch=()):
    return pl.pallas_call(
        kernel,
        out_shape=out,
        in_specs=[VMEM] * n_in,
        out_specs=VMEM,
        scratch_shapes=list(scratch),
        compiler_params=pltpu.CompilerParams(vmem_limit_bytes=limit * 2**20),
        cost_estimate=pl.CostEstimate(flops=flops, bytes_accessed=byts, transcendentals=exps),
    )


def tables(gain, tab_ref):
    p = tab_ref.shape[1]
    gain = jnp.broadcast_to(gain, (tab_ref.shape[2], gain.shape[1])).T
    cosines, sines = [], []
    for half in range(2):
        cos, sin = tab_ref[2 * half], tab_ref[2 * half + 1]
        ga = gain[2 * half * p : (2 * half + 1) * p]
        gb = gain[(2 * half + 1) * p : (2 * half + 2) * p]
        cosines += [ga * cos, gb * cos]
        sines += [-gb * sin, ga * sin]
    return jnp.concatenate(cosines, axis=0), jnp.concatenate(sines, axis=0)


def led_by(lead, n):
    return [[(lead + i) % n for i in range(n)]]


def turned(u, cos, sin):
    hd = u.shape[0]
    p = hd // 4
    swapped = jnp.concatenate([u[p : 2 * p], u[:p], u[3 * p :], u[2 * p : 3 * p]], axis=0)
    inv = lax.rsqrt(jnp.sum(u * u, axis=0, keepdims=True) * (1.0 / hd) + 1e-6)
    return (u * inv) * cos + (swapped * inv) * sin


NT = (((1,), (1,)), ((), ()))


def kv_kernel(copies, x_ref, wk_ref, wv_ref, gain_ref, tab_ref, out_ref):
    x = x_ref[...]
    k = lax.dot_general(wk_ref[...], x, NT, preferred_element_type=F32)
    v = lax.dot_general(wv_ref[...], x, NT, preferred_element_type=F32)
    kt = turned(k.astype(BF16).astype(F32), *tables(gain_ref[1:2], tab_ref)).astype(BF16)
    both = jnp.concatenate([kt, v.astype(BF16)], axis=0)
    for i in range(copies):
        out_ref[i] = both


def q_kernel(x_ref, w_ref, gain_ref, tab_ref, out_ref):
    q = jnp.dot(x_ref[...], w_ref[...], preferred_element_type=F32)
    qt = q.astype(BF16).astype(F32).T
    hd = gain_ref.shape[1]
    both = tables(gain_ref[0:1], tab_ref)
    for h in range(qt.shape[0] // hd):
        rows = slice(h * hd, (h + 1) * hd)
        out_ref[rows] = turned(qt[rows], *both).astype(BF16)


def attend_kernel(hd, zp_ref, q_ref, kv_ref, out_ref, k_ref, v_ref, s_ref):
    n_q, qc, rows = q_ref.shape
    n_pair, heads = n_q // 2, qc // hd
    n_k = kv_ref.shape[0]
    n_keys = n_k * rows
    spots = zp_ref[0], 1 - zp_ref[0]
    step = n_keys // 2
    scale = hd**-0.5 * LOG2E
    for j in range(n_k):
        k_ref[j * rows : (j + 1) * rows, :] = kv_ref[j, :hd, :].astype(F32).T.astype(BF16)
        v_ref[16:, j * rows : (j + 1) * rows] = kv_ref[j, hd:, :]
    v_ref[:16, :] = jnp.ones((16, n_keys), BF16)

    def score(i, h, slot):
        top = None
        q = jnp.concatenate(
            [q_ref[2 * i + b, h * hd : (h + 1) * hd, :] for b in range(2)], axis=1
        )
        for c in range(0, n_keys, step):
            s = jnp.dot(k_ref[c : c + step, :], q, preferred_element_type=F32)
            s_ref[slot, c : c + step] = s
            part = jnp.max(s.reshape(step // 8, 8, 2 * rows), axis=0)
            top = part if top is None else jnp.maximum(top, part)
        return (jnp.max(top, axis=0, keepdims=True) * scale).astype(BF16).astype(F32)

    def pair(i, top):
        tops, sums = [], []
        for h in range(heads):
            if h + 1 < heads:
                later = score(i, h + 1, (h + 1) % 2)
            else:
                later = score(jnp.minimum(i + 1, n_pair - 1), 0, 0)
            o = 0.0
            for c in range(0, n_keys, step):
                p = jnp.exp2(s_ref[h % 2, c : c + step] * scale - top).astype(BF16)
                o += jnp.dot(v_ref[:, c : c + step], p, preferred_element_type=F32)
            tops.append(top)
            sums.append(o[:1])
            for b in range(2):
                out_ref[2 * i + spots[b], h * hd : (h + 1) * hd, :] = o[
                    16:, b * rows : (b + 1) * rows
                ].astype(BF16)
            top = later
        total = jnp.concatenate(sums, axis=0)
        hi = total.astype(BF16).astype(F32)
        stats = jnp.concatenate(tops + [hi, total - hi, jnp.zeros_like(total)], axis=0).astype(BF16)
        for b in range(2):
            out_ref[2 * i + spots[b], qc:, :] = stats[:, b * rows : (b + 1) * rows]
        return top

    lax.fori_loop(0, n_pair, pair, score(0, 0, 0))


def mix_kernel(hd, n_tp, got_ref, w_ref, out_ref, mixed_ref):
    parts, _, rows = got_ref.shape
    qc = w_ref.shape[0]
    heads = qc // hd
    st = [got_ref[i, qc:, :].astype(F32) for i in range(parts)]
    top = functools.reduce(jnp.maximum, [s[:heads] for s in st])
    factor = [jnp.exp2(s[:heads] - top) for s in st]
    total = functools.reduce(
        jnp.add,
        [f * (s[heads : 2 * heads] + s[2 * heads : 3 * heads]) for f, s in zip(factor, st)],
    )
    for h in range(heads):
        acc = 0.0
        for i in range(parts):
            acc += got_ref[i, h * hd : (h + 1) * hd, :].astype(F32) * factor[i][h : h + 1]
        mixed_ref[h * hd : (h + 1) * hd, :] = acc / total[h : h + 1]
    mixed = mixed_ref[...].T.astype(BF16)
    out = jnp.dot(mixed, w_ref[...], preferred_element_type=F32).astype(BF16)
    each = rows // n_tp
    for t in range(n_tp):
        to = (OUT_LEAD + t) % n_tp
        at = (to % 2 + C_LEAD) % 2 * (n_tp // 2) + (X_LEAD - to // 2) % (n_tp // 2)
        out_ref[t] = out[at * each : (at + 1) * each]


def body(tokens_in, w_query, w_key, w_value, w_out, q_gain, k_gain):
    hd = q_gain.shape[0]
    qc = w_query.shape[1]
    mine, d = tokens_in.shape
    n_tp = lax.axis_size(TP)
    rows = mine * n_tp
    n_k = lax.axis_size("zq")
    n_q = lax.axis_size(("zp", "y"))
    heads = qc // hd

    n_x, n_c = lax.axis_size("x"), lax.axis_size("c")
    lane = jnp.arange(rows, dtype=jnp.int32)
    core_of, x_of, row_of = (lane // (n_x * mine) + C_LEAD) % n_c, (X_LEAD - lane // mine) % n_x, lane % mine
    position = lax.axis_index(SP) * rows + (x_of * n_c + core_of) * mine + row_of
    pairs = hd // 4
    freq = 10000.0 ** (-jnp.arange(pairs, dtype=F32) / pairs)
    grid = jnp.stack([position // GRID_W, position % GRID_W]).astype(F32)
    angle = grid[:, None, :] * freq[None, :, None]
    tab = jnp.stack([jnp.cos(angle), jnp.sin(angle)], axis=1).reshape(4, pairs, rows)
    gains = jnp.stack([q_gain, k_gain])
    tokens_in, tab, gains = lax.optimization_barrier((tokens_in, tab, gains))
    sent = jnp.broadcast_to(tokens_in[None], (lax.axis_size("x"), mine, d))
    tokens = lax.all_to_all(sent, "x", 0, 0, tiled=True, axis_index_groups=[[(X_LEAD - i) % n_x for i in range(n_x)]])
    tokens = lax.all_gather(tokens, "c", axis=0, axis_index_groups=led_by(C_LEAD, n_c)).reshape(rows, d)

    query = call(
        q_kernel,
        jax.ShapeDtypeStruct((qc, rows), BF16),
        4,
        2 * rows * d * qc,
        2 * d * (rows + qc),
    )(tokens, w_query, gains, tab)
    other = lax.ppermute(query, "zp", [(0, 1), (1, 0)])
    kv = call(
        functools.partial(kv_kernel, n_k),
        jax.ShapeDtypeStruct((n_k, 2 * hd, rows), BF16),
        5,
        2 * rows * d * 2 * hd,
        2 * d * (rows + 2 * hd),
    )(tokens, w_key.T, w_value.T, gains, tab)
    kv = lax.all_to_all(kv, "zq", 0, 0, tiled=True, axis_index_groups=led_by(Z_LEAD, n_k))
    query = lax.all_gather(
        jnp.stack([query, other]), "y", axis=0, tiled=True, axis_index_groups=[list(Y_ORDER)]
    )
    part = pl.pallas_call(
        functools.partial(attend_kernel, hd),
        out_shape=jax.ShapeDtypeStruct((n_q, qc + 16, rows), BF16),
        in_specs=[pl.BlockSpec(memory_space=pltpu.SMEM), VMEM, VMEM],
        out_specs=VMEM,
        scratch_shapes=[
            pltpu.VMEM((n_k * rows, hd), BF16),
            pltpu.VMEM((hd + 16, n_k * rows), BF16),
            pltpu.VMEM((2, n_k * rows, 2 * rows), F32),
        ],
        compiler_params=pltpu.CompilerParams(vmem_limit_bytes=32 * 2**20),
        cost_estimate=pl.CostEstimate(
            flops=4 * heads * n_q * rows * n_k * rows * hd,
            bytes_accessed=4 * n_q * qc * rows,
            transcendentals=heads * n_q * rows * n_k * rows,
        ),
    )(lax.axis_index("zp").astype(jnp.int32)[None], query, kv)
    got = lax.all_to_all(
        part, ("y", "zp"), 0, 0, tiled=True, axis_index_groups=[[2 * y + p for y in Y_ORDER for p in range(2)]]
    )

    partial = call(
        functools.partial(mix_kernel, hd, n_tp),
        jax.ShapeDtypeStruct((n_tp, mine, d), BF16),
        2,
        2 * rows * qc * d,
        2 * d * (rows + qc),
        scratch=(pltpu.VMEM((qc, rows), F32),),
    )(got, w_out)
    got = lax.all_to_all(
        partial, TP, 0, 0, tiled=True, axis_index_groups=led_by(OUT_LEAD, n_tp)
    )
    return got.astype(F32).sum(axis=0).astype(BF16)


def solution(mesh):
    finer = Mesh(mesh.devices.reshape(8, 2, 4, mesh.shape["tp"] // 2, 2), ALL)

    return jax.shard_map(
        body,
        mesh=finer,
        in_specs=(
            P(ALL, None),
            P(None, TP),
            P(None, TP),
            P(None, TP),
            P(TP, None),
            P(),
            P(),
        ),
        out_specs=P(ALL, None),
        check_vma=False,
    )
```

```python
import functools

import jax
import jax.numpy as jnp
from jax import lax
from jax.experimental import pallas as pl
from jax.experimental.pallas import tpu as pltpu
from jax.sharding import Mesh
from jax.sharding import PartitionSpec as P


F32, BF16 = jnp.float32, jnp.bfloat16
GRID_W = 64
SP = ("zq", "zp", "y")
TP = ("x", "c")
ALL = SP + TP
LOG2E = 1.4426950408889634
C_LEAD, OUT_LEAD, X_LEAD, Z_LEAD = 1, 5, 2, 5
Y_ORDER = 2, 1, 0, 3
VMEM = pl.BlockSpec(memory_space=pltpu.VMEM)


def call(kernel, out, n_in, flops, byts, exps=0, limit=16, scratch=()):
    return pl.pallas_call(
        kernel,
        out_shape=out,
        in_specs=[VMEM] * n_in,
        out_specs=VMEM,
        scratch_shapes=list(scratch),
        compiler_params=pltpu.CompilerParams(vmem_limit_bytes=limit * 2**20),
        cost_estimate=pl.CostEstimate(flops=flops, bytes_accessed=byts, transcendentals=exps),
    )


def tables(gain, tab_ref):
    p = tab_ref.shape[1]
    gain = jnp.broadcast_to(gain, (tab_ref.shape[2], gain.shape[1])).T
    cosines, sines = [], []
    for half in range(2):
        cos, sin = tab_ref[2 * half], tab_ref[2 * half + 1]
        ga = gain[2 * half * p : (2 * half + 1) * p]
        gb = gain[(2 * half + 1) * p : (2 * half + 2) * p]
        cosines += [ga * cos, gb * cos]
        sines += [-gb * sin, ga * sin]
    return jnp.concatenate(cosines, axis=0), jnp.concatenate(sines, axis=0)


def led_by(lead, n):
    return [[(lead + i) % n for i in range(n)]]


def turned(u, cos, sin):
    hd = u.shape[0]
    p = hd // 4
    swapped = jnp.concatenate([u[p : 2 * p], u[:p], u[3 * p :], u[2 * p : 3 * p]], axis=0)
    inv = lax.rsqrt(jnp.sum(u * u, axis=0, keepdims=True) * (1.0 / hd) + 1e-6)
    return (u * inv) * cos + (swapped * inv) * sin


NT = (((1,), (1,)), ((), ()))


def kv_kernel(copies, x_ref, wk_ref, wv_ref, gain_ref, tab_ref, out_ref):
    x = x_ref[...]
    k = lax.dot_general(wk_ref[...], x, NT, preferred_element_type=F32)
    v = lax.dot_general(wv_ref[...], x, NT, preferred_element_type=F32)
    kt = turned(k.astype(BF16).astype(F32), *tables(gain_ref[1:2], tab_ref)).astype(BF16)
    both = jnp.concatenate([kt, v.astype(BF16)], axis=0)
    for i in range(copies):
        out_ref[i] = both


def q_kernel(x_ref, w_ref, gain_ref, tab_ref, out_ref):
    q = jnp.dot(x_ref[...], w_ref[...], preferred_element_type=F32)
    qt = q.astype(BF16).astype(F32).T
    hd = gain_ref.shape[1]
    both = tables(gain_ref[0:1], tab_ref)
    for h in range(qt.shape[0] // hd):
        rows = slice(h * hd, (h + 1) * hd)
        out_ref[rows] = turned(qt[rows], *both).astype(BF16)


def attend_kernel(hd, zp_ref, q_ref, kv_ref, out_ref, k_ref, v_ref, s_ref):
    n_q, qc, rows = q_ref.shape
    n_pair, heads = n_q // 2, qc // hd
    n_k = kv_ref.shape[0]
    n_keys = n_k * rows
    spots = zp_ref[0], 1 - zp_ref[0]
    step = n_keys // 2
    scale = hd**-0.5 * LOG2E
    for j in range(n_k):
        k_ref[j * rows : (j + 1) * rows, :] = kv_ref[j, :hd, :].astype(F32).T.astype(BF16)
        v_ref[16:, j * rows : (j + 1) * rows] = kv_ref[j, hd:, :]
    v_ref[:16, :] = jnp.ones((16, n_keys), BF16)

    def score(i, h, slot):
        top = None
        q = jnp.concatenate(
            [q_ref[2 * i + b, h * hd : (h + 1) * hd, :] for b in range(2)], axis=1
        )
        for c in range(0, n_keys, step):
            s = jnp.dot(k_ref[c : c + step, :], q, preferred_element_type=F32)
            s_ref[slot, c : c + step] = s
            part = jnp.max(s.reshape(step // 8, 8, 2 * rows), axis=0)
            top = part if top is None else jnp.maximum(top, part)
        return (jnp.max(top, axis=0, keepdims=True) * scale).astype(BF16).astype(F32)

    def pair(i, top):
        tops, sums = [], []
        for h in range(heads):
            if h + 1 < heads:
                later = score(i, h + 1, (h + 1) % 2)
            else:
                later = score(jnp.minimum(i + 1, n_pair - 1), 0, 0)
            o = 0.0
            for c in range(0, n_keys, step):
                p = jnp.exp2(s_ref[h % 2, c : c + step] * scale - top).astype(BF16)
                o += jnp.dot(v_ref[:, c : c + step], p, preferred_element_type=F32)
            tops.append(top)
            sums.append(o[:1])
            for b in range(2):
                out_ref[n_pair * spots[b] + i, h * hd : (h + 1) * hd, :] = o[
                    16:, b * rows : (b + 1) * rows
                ].astype(BF16)
            top = later
        total = jnp.concatenate(sums, axis=0)
        hi = total.astype(BF16).astype(F32)
        stats = jnp.concatenate(tops + [hi, total - hi, jnp.zeros_like(total)], axis=0).astype(BF16)
        for b in range(2):
            out_ref[n_pair * spots[b] + i, qc:, :] = stats[:, b * rows : (b + 1) * rows]
        return top

    lax.fori_loop(0, n_pair, pair, score(0, 0, 0))


def mix_kernel(hd, n_tp, got_ref, w_ref, out_ref, mixed_ref):
    parts, _, rows = got_ref.shape
    qc = w_ref.shape[0]
    heads = qc // hd
    st = [got_ref[i, qc:, :].astype(F32) for i in range(parts)]
    top = functools.reduce(jnp.maximum, [s[:heads] for s in st])
    factor = [jnp.exp2(s[:heads] - top) for s in st]
    total = functools.reduce(
        jnp.add,
        [f * (s[heads : 2 * heads] + s[2 * heads : 3 * heads]) for f, s in zip(factor, st)],
    )
    for h in range(heads):
        acc = 0.0
        for i in range(parts):
            acc += got_ref[i, h * hd : (h + 1) * hd, :].astype(F32) * factor[i][h : h + 1]
        mixed_ref[h * hd : (h + 1) * hd, :] = acc / total[h : h + 1]
    mixed = mixed_ref[...].T.astype(BF16)
    out = jnp.dot(mixed, w_ref[...], preferred_element_type=F32).astype(BF16)
    each = rows // n_tp
    for t in range(n_tp):
        to = (OUT_LEAD + t) % n_tp
        at = (to % 2 + C_LEAD) % 2 * (n_tp // 2) + (X_LEAD - to // 2) % (n_tp // 2)
        out_ref[t] = out[at * each : (at + 1) * each]


def body(tokens_in, w_query, w_key, w_value, w_out, q_gain, k_gain):
    hd = q_gain.shape[0]
    qc = w_query.shape[1]
    mine, d = tokens_in.shape
    n_tp = lax.axis_size(TP)
    rows = mine * n_tp
    n_k = lax.axis_size("zq")
    n_q = lax.axis_size(("zp", "y"))
    heads = qc // hd

    n_x, n_c = lax.axis_size("x"), lax.axis_size("c")
    lane = jnp.arange(rows, dtype=jnp.int32)
    core_of, x_of, row_of = (lane // (n_x * mine) + C_LEAD) % n_c, (X_LEAD - lane // mine) % n_x, lane % mine
    position = lax.axis_index(SP) * rows + (x_of * n_c + core_of) * mine + row_of
    pairs = hd // 4
    freq = 10000.0 ** (-jnp.arange(pairs, dtype=F32) / pairs)
    grid = jnp.stack([position // GRID_W, position % GRID_W]).astype(F32)
    angle = grid[:, None, :] * freq[None, :, None]
    tab = jnp.stack([jnp.cos(angle), jnp.sin(angle)], axis=1).reshape(4, pairs, rows)
    gains = jnp.stack([q_gain, k_gain])
    tokens_in, tab, gains = lax.optimization_barrier((tokens_in, tab, gains))
    sent = jnp.broadcast_to(tokens_in[None], (lax.axis_size("x"), mine, d))
    tokens = lax.all_to_all(sent, "x", 0, 0, tiled=True, axis_index_groups=[[(X_LEAD - i) % n_x for i in range(n_x)]])
    tokens = lax.all_gather(tokens, "c", axis=0, axis_index_groups=led_by(C_LEAD, n_c)).reshape(rows, d)

    query = call(
        q_kernel,
        jax.ShapeDtypeStruct((qc, rows), BF16),
        4,
        2 * rows * d * qc,
        2 * d * (rows + qc),
    )(tokens, w_query, gains, tab)
    other = lax.ppermute(query, "zp", [(0, 1), (1, 0)])
    kv = call(
        functools.partial(kv_kernel, n_k),
        jax.ShapeDtypeStruct((n_k, 2 * hd, rows), BF16),
        5,
        2 * rows * d * 2 * hd,
        2 * d * (rows + 2 * hd),
    )(tokens, w_key.T, w_value.T, gains, tab)
    kv = lax.all_to_all(kv, "zq", 0, 0, tiled=True, axis_index_groups=led_by(Z_LEAD, n_k))
    query = lax.all_gather(
        jnp.stack([query, other]), "y", axis=0, tiled=True, axis_index_groups=[list(Y_ORDER)]
    )
    part = pl.pallas_call(
        functools.partial(attend_kernel, hd),
        out_shape=jax.ShapeDtypeStruct((n_q, qc + 16, rows), BF16),
        in_specs=[pl.BlockSpec(memory_space=pltpu.SMEM), VMEM, VMEM],
        out_specs=VMEM,
        scratch_shapes=[
            pltpu.VMEM((n_k * rows, hd), BF16),
            pltpu.VMEM((hd + 16, n_k * rows), BF16),
            pltpu.VMEM((2, n_k * rows, 2 * rows), F32),
        ],
        compiler_params=pltpu.CompilerParams(vmem_limit_bytes=32 * 2**20),
        cost_estimate=pl.CostEstimate(
            flops=4 * heads * n_q * rows * n_k * rows * hd,
            bytes_accessed=4 * n_q * qc * rows,
            transcendentals=heads * n_q * rows * n_k * rows,
        ),
    )(lax.axis_index("zp").astype(jnp.int32)[None], query, kv)
    got = lax.all_to_all(
        part, ("y", "zp"), 0, 0, tiled=True, axis_index_groups=[[2 * y + p for p in range(2) for y in Y_ORDER]]
    )

    partial = call(
        functools.partial(mix_kernel, hd, n_tp),
        jax.ShapeDtypeStruct((n_tp, mine, d), BF16),
        2,
        2 * rows * qc * d,
        2 * d * (rows + qc),
        scratch=(pltpu.VMEM((qc, rows), F32),),
    )(got, w_out)
    got = lax.all_to_all(
        partial, TP, 0, 0, tiled=True, axis_index_groups=led_by(OUT_LEAD, n_tp)
    )
    return got.astype(F32).sum(axis=0).astype(BF16)


def solution(mesh):
    finer = Mesh(mesh.devices.reshape(8, 2, 4, mesh.shape["tp"] // 2, 2), ALL)

    return jax.shard_map(
        body,
        mesh=finer,
        in_specs=(
            P(ALL, None),
            P(None, TP),
            P(None, TP),
            P(None, TP),
            P(TP, None),
            P(),
            P(),
        ),
        out_specs=P(ALL, None),
        check_vma=False,
    )
```
